32 devices in a mesh: sp: 16 (over z, y, x), tp: 2 (over core).
Axes of the slice: x: 2, y: 2, z: 4, core: 2. Of those that a mesh axis runs over, the one named last changes fastest.
Arguments:
- tokens: bfloat16 [2048, 2048], P('sp'), may hold values from -6 to 6
- in_gain: bfloat16 [2048], replicated, may hold values from 0.099609375 to 1.8984375
- w_value: bfloat16 [2048, 4096], P('sp', 'tp'), may hold values from -0.125 to 0.125
- w_gate: bfloat16 [2048, 4096], P('sp', 'tp'), may hold values from -0.125 to 0.125
- w_in_key: bfloat16 [2048, 1024], P('sp', 'tp'), may hold values from -0.125 to 0.125
- w_read: bfloat16 [2048, 1024], P('sp', 'tp'), may hold values from -0.125 to 0.125
- w_step_fwd: bfloat16 [2048, 64], P('sp', 'tp'), may hold values from -0.25 to 0.25
- w_step_bwd: bfloat16 [2048, 64], P('sp', 'tp'), may hold values from -0.25 to 0.25
- conv_value: bfloat16 [5, 4096], P(None, 'tp'), may hold values from -2.5 to 2.5
- conv_key: bfloat16 [5, 1024], P(None, 'tp'), may hold values from -2.5 to 2.5
- conv_read: bfloat16 [5, 1024], P(None, 'tp'), may hold values from -2.5 to 2.5
- step_bias: float32 [2, 64], P(None, 'tp'), may hold values from -4 to -2
- rate: float32 [2, 64], P(None, 'tp'), may hold values from 0 to 1, as said below
- norm_gain: bfloat16 [4096], P('tp'), may hold values from 0.099609375 to 1.8984375
- w_out: bfloat16 [4096, 2048], P('tp', 'sp'), may hold values from -0.09375 to 0.09375
Outputs:
- mixed: bfloat16 [2048, 2048], P('sp')
The draws below stay inside these ranges and needn't reach their ends.
Inputs may be any that keep to these rules, and one draw needn't show every extreme that they name: `rate`: positive decay rates, one per head and direction.
All inputs are finite; a program needn't handle non-finite values.
Results may differ from the reference program's by a relative error of at most 0.018.
Values may be sent and summed in bfloat16 or wider, within the bound.
A program may use at most 128 MiB of HBM per device.

```python
import math
import jax
import jax.numpy as jnp
from jax import lax

D = 2048
HEADS = 64
HEAD_DIM = 64
GROUPS = 8
STATE = 128
KERNEL = 5
BLOCK = 128
INNER = 4096
SEQ = 2048
N_TP = 2


def draw_rate(key, part):
    chooser, fast_key, slow_key = jax.random.split(jax.random.fold_in(key, 7), 3)
    fast_share = 0.5
    picked = jax.random.uniform(chooser, (2, HEADS), jnp.float32) < fast_share
    fast_rates = jnp.exp(jax.random.uniform(fast_key, (2, HEADS), jnp.float32, math.log(0.01), math.log(1.0 / 30.0))) / 0.4
    slow_rates = jnp.exp(jax.random.uniform(slow_key, (2, HEADS), jnp.float32, math.log(0.5), math.log(2.0))) / (0.4 * SEQ)
    return jnp.where(picked, fast_rates, slow_rates).astype(jnp.float32)


def steps_of(own_key, extent, pieces, smallest, largest):
    loudness = 1.0
    for position, blocks in pieces:
        steps = jax.random.uniform(jax.random.fold_in(jax.random.fold_in(own_key, 6), position), (blocks,), jnp.float32, smallest / len(pieces), largest / len(pieces))
        loudness = loudness * jnp.repeat(jnp.exp(steps), extent[position] // blocks).reshape((-1,) + (1,) * (len(extent) - 1 - position))
    return loudness


def bell_draw(own_key, dims, deviation, limit, cuts=(), dtype=jnp.bfloat16):
    entries = deviation * jax.random.normal(own_key, dims, jnp.float32)
    if cuts:
        entries = entries * steps_of(own_key, dims, cuts, -0.22, 0.18)
    return jnp.clip(entries, -limit, limit).astype(dtype)


def setup_inputs(seed: int = 0) -> dict:
    seeds = jax.random.split(jax.random.key(seed), 16)
    return {
        "tokens": bell_draw(seeds[0], (SEQ, D), 1.0, 6.0, ((0, 16),)),
        "in_gain": jnp.clip(1.0 + 0.18 * jax.random.normal(seeds[1], (D,), jnp.float32), 0.099609375, 1.8984375).astype(jnp.bfloat16),
        "w_value": bell_draw(seeds[2], (D, INNER), D ** -0.5, 0.125, ((0, 16), (1, 2))),
        "w_gate": bell_draw(seeds[3], (D, INNER), D ** -0.5, 0.125, ((0, 16), (1, 2))),
        "w_in_key": bell_draw(seeds[4], (D, GROUPS * STATE), D ** -0.5, 0.125, ((0, 16), (1, 2))),
        "w_read": bell_draw(seeds[5], (D, GROUPS * STATE), D ** -0.5, 0.125, ((0, 16), (1, 2))),
        "w_step_fwd": bell_draw(seeds[6], (D, HEADS), (D // 4) ** -0.5, 0.25, ((0, 16), (1, 2))),
        "w_step_bwd": bell_draw(seeds[7], (D, HEADS), (D // 4) ** -0.5, 0.25, ((0, 16), (1, 2))),
        "conv_value": bell_draw(seeds[8], (KERNEL, INNER), KERNEL ** -0.5, 2.5, ((1, 2),)),
        "conv_key": bell_draw(seeds[9], (KERNEL, GROUPS * STATE), KERNEL ** -0.5, 2.5, ((1, 2),)),
        "conv_read": bell_draw(seeds[10], (KERNEL, GROUPS * STATE), KERNEL ** -0.5, 2.5, ((1, 2),)),
        "step_bias": jnp.clip(-4.0 + 2.0 * jax.random.uniform(seeds[11], (2, HEADS), jnp.float32) ** steps_of(seeds[11], (2, HEADS), ((1, 2),), -0.2, 0.2), -4.0, -2.0),
        "rate": draw_rate(jax.random.fold_in(seeds[15], 71), 0),
        "norm_gain": jnp.clip(1.0 + 0.18 * jax.random.normal(seeds[13], (INNER,), jnp.float32), 0.099609375, 1.8984375).astype(jnp.bfloat16),
        "w_out": bell_draw(seeds[14], (INNER, D), INNER ** -0.5, 0.09375, ((0, 2), (1, 16))),
    }


EPSILON = 1e-05
FULL_PRECISION = lax.Precision.HIGHEST

def normalize(tensor, gain):
    return tensor * lax.rsqrt(lax.optimization_barrier(jnp.mean(tensor * tensor, -1, keepdims=True)) + EPSILON) * gain

def centred(projected, kernel_taps):
    tap_count = kernel_taps.shape[0]
    half_reach = (tap_count - 1) // 2
    length = projected.shape[0]
    padded = jnp.pad(projected.astype(jnp.float32), ((half_reach, half_reach), (0, 0)))
    summed = jnp.zeros(projected.shape, jnp.float32)
    for offset in range(tap_count):
        summed = summed + padded[offset:offset + length] * kernel_taps[offset].astype(jnp.float32)
    return jax.nn.silu(summed).astype(jnp.bfloat16)

def block_parts(values, step_size, log_decay, in_keys):
    per_group = values.shape[1] // in_keys.shape[1]
    cumulative = jnp.cumsum(log_decay, axis=0)
    log_total = cumulative[-1]
    weighting = jnp.exp(log_total[None, :] - cumulative) * step_size
    key_heads = jnp.repeat(in_keys.astype(jnp.float32), per_group, axis=1)
    scaled = (values.astype(jnp.float32) * weighting[:, :, None]).astype(jnp.bfloat16).astype(jnp.float32)
    injected = jnp.einsum('jhn,jhp->hpn', key_heads, scaled, precision=FULL_PRECISION)
    return (cumulative, jnp.exp(log_total), injected)

def block_step(memory, inputs):
    values, step_size, log_decay, in_keys, read_in = inputs
    per_group = values.shape[1] // in_keys.shape[1]
    cumulative, damping, injected = block_parts(values, step_size, log_decay, in_keys)
    scores = jnp.einsum('ign,jgn->ijg', read_in.astype(jnp.float32), in_keys.astype(jnp.float32), precision=FULL_PRECISION)
    scores = jnp.repeat(scores, per_group, axis=2)
    length = values.shape[0]
    below_mask = (jnp.arange(length)[:, None] >= jnp.arange(length)[None, :])[:, :, None]
    gaps = jnp.where(below_mask, cumulative[:, None, :] - cumulative[None, :, :], -jnp.inf)
    weights = (scores * jnp.exp(gaps) * step_size[None, :, :]).astype(jnp.bfloat16).astype(jnp.float32)
    within = jnp.einsum('ijh,jhp->ihp', weights, values.astype(jnp.float32), precision=FULL_PRECISION)
    read_heads = jnp.repeat(read_in.astype(jnp.float32), per_group, axis=1)
    carried = jnp.einsum('ihn,hpn->ihp', read_heads, memory, precision=FULL_PRECISION) * jnp.exp(cumulative)[:, :, None]
    memory = damping[:, None, None] * memory + injected
    return (memory, within + carried)

def sweep(values, step_size, log_decay, in_keys, read_in, memory):
    blocks = values.shape[0] // BLOCK

    def blocked(tensor):
        return tensor.reshape((blocks, BLOCK) + tensor.shape[1:])
    memory, swept = lax.scan(block_step, memory, (blocked(values), blocked(step_size), blocked(log_decay), blocked(in_keys), blocked(read_in)))
    return (swept.reshape((blocks * BLOCK,) + swept.shape[2:]), memory)

def reference(tokens, in_gain, w_value, w_gate, w_in_key, w_read, w_step_fwd, w_step_bwd, conv_value, conv_key, conv_read, step_bias, rate, norm_gain, w_out):
    normed = normalize(tokens.astype(jnp.float32), in_gain.astype(jnp.float32)).astype(jnp.bfloat16)

    def project(weight):
        return jnp.dot(normed, weight, preferred_element_type=jnp.float32).astype(jnp.bfloat16)
    length = tokens.shape[0]
    values = centred(project(w_value), conv_value).reshape(length, HEADS, HEAD_DIM)
    gate_raw = project(w_gate)
    in_keys = centred(project(w_in_key), conv_key).reshape(length, GROUPS, STATE)
    read_in = centred(project(w_read), conv_read).reshape(length, GROUPS, STATE)
    blank = jnp.zeros((HEADS, HEAD_DIM, STATE), jnp.float32)
    summed_heads = jnp.zeros((length, HEADS, HEAD_DIM), jnp.float32)
    for direction, weight in ((0, w_step_fwd), (1, w_step_bwd)):
        step_pre = project(weight).astype(jnp.float32)
        step_size = jax.nn.softplus(step_pre + step_bias[direction].astype(jnp.float32))
        log_decay = -rate[direction].astype(jnp.float32) * step_size
        if direction == 0:
            swept, final_state = sweep(values, step_size, log_decay, in_keys, read_in, blank)
        else:
            swept, final_state = sweep(values[::-1], step_size[::-1], log_decay[::-1], in_keys[::-1], read_in[::-1], blank)
            swept = swept[::-1]
        summed_heads = summed_heads + swept
    gated_out = summed_heads * jax.nn.silu(gate_raw.astype(jnp.float32)).reshape(length, HEADS, HEAD_DIM)
    head_gain = norm_gain.astype(jnp.float32).reshape(HEADS, HEAD_DIM)
    normed_heads = normalize(gated_out, head_gain).astype(jnp.bfloat16).reshape(length, INNER)
    part_width = INNER // N_TP
    result = jnp.zeros((length, D), jnp.float32)
    for tp_part in range(N_TP):
        portion = jnp.dot(normed_heads[:, tp_part * part_width:(tp_part + 1) * part_width], w_out[tp_part * part_width:(tp_part + 1) * part_width], preferred_element_type=jnp.float32)
        result = result + lax.optimization_barrier(portion.astype(jnp.bfloat16)).astype(jnp.float32)
    return result.astype(jnp.bfloat16)
```

```python
import functools
import math

import jax
import jax.numpy as jnp
from jax import lax
from jax.experimental import pallas as pl
from jax.experimental.pallas import tpu as pltpu
from jax.sharding import PartitionSpec as P

HEAD_DIM = 64
STATE = 128
KERNEL = 5
BLOCK = 128


EPSILON = 1e-05
FULL_PRECISION = lax.Precision.HIGHEST


def entering_2(x, axis, combine, identity, reverse):
    length, place = (lax.axis_size(axis), lax.axis_index(axis))
    everything = jax.tree.map(lambda part: lax.all_gather(part, axis), x)
    start = jax.tree.map(
        lambda part, zero: jnp.broadcast_to(jnp.asarray(zero, part.dtype), part.shape), x, identity
    )

    def step(k, before):
        at = length - 1 - k if reverse else k
        reached = at > place if reverse else at < place
        new = combine(before, jax.tree.map(lambda part: part[at], everything))
        return jax.tree.map(lambda a, b: jnp.where(reached, a, b), new, before)

    return lax.fori_loop(0, length, step, start)


def with_halo(cells, sides, width):
    for axis, dim in sides:
        count = lax.axis_size(axis)
        ends = count - 1
        head = lax.slice_in_dim(cells, 0, width, axis=dim)
        tail = lax.slice_in_dim(cells, cells.shape[dim] - width, cells.shape[dim], axis=dim)
        cells = jnp.concatenate(
            [
                lax.ppermute(tail, axis, [(i, (i + 1) % count) for i in range(ends)]),
                cells,
                lax.ppermute(head, axis, [((i + 1) % count, i) for i in range(ends)]),
            ],
            axis=dim,
        )
    return cells


def normalize(tensor, gain):
    return tensor * lax.rsqrt(jnp.mean(tensor * tensor, -1, keepdims=True) + EPSILON) * gain


def block_parts(values, step_size, log_decay, in_keys):
    per_group = values.shape[1] // in_keys.shape[1]
    cumulative = jnp.cumsum(log_decay, axis=0)
    log_total = cumulative[-1]
    weighting = jnp.exp(log_total[None, :] - cumulative) * step_size
    key_heads = jnp.repeat(in_keys, per_group, axis=1)
    scaled = (values.astype(jnp.float32) * weighting[:, :, None]).astype(jnp.bfloat16)
    injected = jnp.einsum("jhn,jhp->hpn", key_heads, scaled, preferred_element_type=jnp.float32)
    return (cumulative, jnp.exp(log_total), injected)


def block_step(memory, inputs):
    values, step_size, cumulative, damping, injected, in_keys, read_in = inputs
    per_group = values.shape[1] // in_keys.shape[1]
    scores = jnp.einsum("ign,jgn->ijg", read_in, in_keys, preferred_element_type=jnp.float32)
    scores = jnp.repeat(scores, per_group, axis=2)
    length = values.shape[0]
    below_mask = (jnp.arange(length)[:, None] >= jnp.arange(length)[None, :])[:, :, None]
    gaps = jnp.where(below_mask, cumulative[:, None, :] - cumulative[None, :, :], -jnp.inf)
    weights = (scores * jnp.exp(gaps) * step_size[None, :, :]).astype(jnp.bfloat16)
    within = jnp.einsum("ijh,jhp->ihp", weights, values, preferred_element_type=jnp.float32)
    read_heads = jnp.repeat(read_in.astype(jnp.float32), per_group, axis=1)
    carried = (
        jnp.einsum("ihn,hpn->ihp", read_heads, memory, precision=FULL_PRECISION)
        * jnp.exp(cumulative)[:, :, None]
    )
    memory = damping[:, None, None] * memory + injected
    return (memory, within + carried)


def blocked(tensor):
    blocks = tensor.shape[0] // BLOCK
    return tensor.reshape((blocks, BLOCK) + tensor.shape[1:])


def sweep(block_inputs, memory):
    memory, swept = lax.scan(block_step, memory, block_inputs)
    return (swept.reshape((swept.shape[0] * swept.shape[1],) + swept.shape[2:]), memory)


def settle(damping_blocks, injected_blocks, memory):

    def advance(memory, inputs):
        return (inputs[0][:, None, None] * memory + inputs[1], None)

    memory, unused = lax.scan(advance, memory, (damping_blocks, injected_blocks))
    return memory


def chain(before_pair, after_pair):
    return (
        before_pair[0] * after_pair[0],
        after_pair[0][:, None, None] * before_pair[1] + after_pair[1],
    )


def entering(damping, final_state, backward):
    identity_pair = (jnp.ones_like(damping), jnp.zeros_like(final_state))
    if backward:
        arrived = entering_2((damping, final_state), "sp", chain, identity_pair, True)
    else:
        arrived = entering_2((damping, final_state), "sp", chain, identity_pair, False)
    return arrived[1]


def body(
    tokens,
    in_gain,
    w_value,
    w_gate,
    w_in_key,
    w_read,
    w_step_fwd,
    w_step_bwd,
    conv_value,
    conv_key,
    conv_read,
    step_bias,
    rate,
    norm_gain,
    w_out,
):
    normed = normalize(tokens.astype(jnp.float32), in_gain.astype(jnp.float32)).astype(jnp.bfloat16)
    weights = (
        lax.all_gather(w_value, "sp", axis=0, tiled=True),
        lax.all_gather(w_gate, "sp", axis=0, tiled=True),
        lax.all_gather(w_in_key, "sp", axis=0, tiled=True),
        lax.all_gather(w_read, "sp", axis=0, tiled=True),
        lax.all_gather(w_step_fwd, "sp", axis=0, tiled=True),
        lax.all_gather(w_step_bwd, "sp", axis=0, tiled=True),
    )
    projected = [
        jnp.dot(normed, weight, preferred_element_type=jnp.float32).astype(jnp.bfloat16)
        for weight in weights
    ]
    value_raw, gate_raw, key_raw, read_raw, pre_fwd, pre_bwd = projected
    value_cols = value_raw.shape[1]
    key_cols = key_raw.shape[1]
    joined = jnp.concatenate([value_raw, key_raw, read_raw], axis=1)
    padded = with_halo(joined, (("sp", 0),), (KERNEL - 1) // 2)
    kernel_taps = jnp.concatenate([conv_value, conv_key, conv_read], axis=1).astype(jnp.float32)
    length = joined.shape[0]
    summed = jnp.zeros(joined.shape, jnp.float32)
    for offset in range(KERNEL):
        summed = summed + padded[offset : offset + length].astype(jnp.float32) * kernel_taps[offset]
    mixed_in = jax.nn.silu(summed).astype(jnp.bfloat16)
    head_count = value_cols // HEAD_DIM
    group_count = key_cols // STATE
    values = mixed_in[:, :value_cols].reshape(length, head_count, HEAD_DIM)
    in_keys = mixed_in[:, value_cols : value_cols + key_cols].reshape(length, group_count, STATE)
    read_in = mixed_in[:, value_cols + key_cols :].reshape(length, group_count, STATE)
    blank = jnp.zeros((head_count, HEAD_DIM, STATE), jnp.float32)
    summed_heads = jnp.zeros(values.shape, jnp.float32)
    for direction, step_pre in ((0, pre_fwd), (1, pre_bwd)):
        step_size = jax.nn.softplus(step_pre.astype(jnp.float32) + step_bias[direction])
        log_decay = -rate[direction] * step_size
        ordered = (values, step_size, log_decay, in_keys, read_in)
        if direction == 1:
            ordered = tuple((tensor[::-1] for tensor in ordered))
        value_blocks, step_blocks, decay_blocks, key_blocks, read_blocks = [
            blocked(tensor) for tensor in ordered
        ]
        cumulative_blocks, damping_blocks, injected_blocks = jax.vmap(block_parts)(
            value_blocks, step_blocks, decay_blocks, key_blocks
        )
        block_inputs = (
            value_blocks,
            step_blocks,
            cumulative_blocks,
            damping_blocks,
            injected_blocks,
            key_blocks,
            read_blocks,
        )
        damping = jnp.exp(jnp.sum(ordered[2], axis=0))
        final_state = settle(damping_blocks, injected_blocks, blank)
        arriving = entering(damping, final_state, direction == 1)
        swept, final_state = sweep(block_inputs, arriving)
        if direction == 1:
            swept = swept[::-1]
        summed_heads = summed_heads + swept
    gated_out = summed_heads * jax.nn.silu(gate_raw.astype(jnp.float32)).reshape(values.shape)
    head_gain = norm_gain.astype(jnp.float32).reshape(head_count, HEAD_DIM)
    normed_heads = normalize(gated_out, head_gain).astype(jnp.bfloat16).reshape(length, value_cols)
    out_whole = lax.all_gather(w_out, "sp", axis=1, tiled=True)
    own_rows = lax.psum_scatter(
        jnp.dot(normed_heads, out_whole, preferred_element_type=jnp.float32).astype(jnp.bfloat16),
        "tp",
        scatter_dimension=0,
        tiled=True,
    )
    return lax.all_gather(own_rows, "tp", axis=0, tiled=True)


F32 = jnp.float32
BF16 = jnp.bfloat16
LANES = 128
VMEM_SPEC = pl.BlockSpec(memory_space=pltpu.VMEM)


def greet(peers):
    barrier = pltpu.get_barrier_semaphore()
    for peer in peers:
        pl.semaphore_signal(
            barrier, inc=1, device_id=peer, device_id_type=pl.DeviceIdType.MESH
        )
    pl.semaphore_wait(barrier, len(peers))


def push(src, dst, send, recv, peer):
    copy = pltpu.make_async_remote_copy(
        src_ref=src,
        dst_ref=dst,
        send_sem=send,
        recv_sem=recv,
        device_id=peer,
        device_id_type=pl.DeviceIdType.MESH,
    )
    copy.start()
    return copy


def gather_kernel(n, q, nrm, wv, wg, wk, wr, ws, wo, tok, wts, wout, ts, tr, ps, pr, ss, sr, ms, mr, os, orr, ls):
    s, t = lax.axis_index("sp"), lax.axis_index("tp")
    z, p = s // q, s % q
    sibling = (s, 1 - t)
    per = n // (wk.shape[1] // LANES)
    half = tok.shape[2]
    depth = wv.shape[0]

    def peer(k):
        return lax.rem(s + k, n)

    def at(dz, dp):
        return lax.rem(z + dz, q) * q + lax.rem(p + dp, q)

    greet([(peer(k), t) for k in range(1, n)] + [sibling])
    rows = pl.ds(pl.multiple_of(t * half, half), half)
    first = []
    for dz in range(1, q):
        first.append(push(nrm.at[rows], tok.at[s, t], ts.at[dz], tr.at[dz], (at(dz, 0), t)))
    own = []
    for c in range(2):
        copy = pltpu.make_async_copy(nrm.at[pl.ds(c * half, half)], tok.at[s, c], ls.at[c])
        copy.start()
        own.append(copy)
    mine = pl.ds(pl.multiple_of(s * depth, depth), depth)

    def pieces(j):
        cols = pl.ds(pl.multiple_of(j * LANES, LANES), LANES)
        group = pl.ds(pl.multiple_of((j // per) * LANES, LANES), LANES)
        return (wv.at[:, cols], wg.at[:, cols], wk.at[:, group], wr.at[:, group], ws.at[j])

    def target(i):
        return wts.at[mine, pl.ds(i * LANES, LANES)]

    second = []
    for dp in range(1, q):
        second.append(push(nrm.at[rows], tok.at[s, t], ps.at[0, dp], pr.at[0, dp], (at(0, dp), t)))
    sent = []
    for k in range(1, n):
        for i, piece in enumerate(pieces(peer(k))):
            sent.append(push(piece, target(i), ms.at[k, i], mr.at[k, i], (peer(k), t)))
    for i, piece in enumerate(pieces(s)):
        copy = pltpu.make_async_copy(piece, target(i), ls.at[2 + i])
        copy.start()
        own.append(copy)
    last = []
    for dz in range(1, q):
        first[dz - 1].wait_recv()
        src = at(q - dz, 0)
        for dp in range(1, q):
            second.append(
                push(tok.at[src, t], tok.at[src, t], ps.at[dz, dp], pr.at[dz, dp], (at(0, dp), t))
            )
        last.append(push(tok.at[src, t], tok.at[src, t], ss.at[dz, 0], sr.at[dz, 0], sibling))
    outs = []
    col = pl.ds(pl.multiple_of(p * LANES, LANES), LANES)
    for dp in range(1, q):
        outs.append(push(wo, wout.at[:, col], os.at[dp], orr.at[dp], (at(0, dp), t)))
    copy = pltpu.make_async_copy(wo, wout.at[:, col], ls.at[7])
    copy.start()
    own.append(copy)
    for dz in range(q):
        for dp in range(1, q):
            second[dz * (q - 1) + dp - 1].wait_recv()
            src = at(q - dz, q - dp)
            last.append(push(tok.at[src, t], tok.at[src, t], ss.at[dz, dp], sr.at[dz, dp], sibling))
    for copy in own:
        copy.wait()
    for copy in first + second:
        copy.wait_send()
    for copy in sent + last + outs:
        copy.wait()


def gather(n, q, nrm, wv, wg, wk, wr, ws, wo):
    dma = pltpu.SemaphoreType.DMA
    length, width = nrm.shape
    return pl.pallas_call(
        functools.partial(gather_kernel, n, q),
        out_shape=(
            jax.ShapeDtypeStruct((n, 2, length // 2, width), BF16),
            jax.ShapeDtypeStruct((n * wv.shape[0], 5 * LANES), BF16),
            jax.ShapeDtypeStruct((wo.shape[0], q * LANES), BF16),
        ),
        in_specs=[VMEM_SPEC] * 7,
        out_specs=(VMEM_SPEC,) * 3,
        scratch_shapes=[
            dma((q,)), dma((q,)), dma((q, q)), dma((q, q)), dma((q, q)), dma((q, q)),
            dma((n, 5)), dma((n, 5)), dma((q,)), dma((q,)), dma((8,)),
        ],
        compiler_params=pltpu.CompilerParams(
            collective_id=0, has_side_effects=True, vmem_limit_bytes=48 << 20
        ),
        name="gather",
    )(nrm, wv, wg, wk, wr, ws, wo)


def spread_kernel(q, nh, full, s1, r1, s2, r2, ls):
    s, t = lax.axis_index("sp"), lax.axis_index("tp")
    z, p = s // q, s % q

    def at(dz, dp):
        return lax.rem(z + dz, q) * q + lax.rem(p + dp, q)

    def col(i):
        return pl.ds(pl.multiple_of(i * LANES, LANES), LANES)

    greet([(at(0, d), t) for d in range(1, q)] + [(at(d, 0), t) for d in range(1, q)])
    first = []
    for dp in range(1, q):
        first.append(
            push(
                nh.at[:, lax.rem(p + dp, q)], full.at[:, :, col(s)],
                s1.at[dp], r1.at[dp], (at(0, dp), t),
            )
        )
    own = pltpu.make_async_copy(nh.at[:, p], full.at[:, :, col(s)], ls.at[0])
    own.start()
    second = []
    for dz in range(1, q):
        second.append(
            push(nh.at[:, p], full.at[:, :, col(s)], s2.at[dz, 0], r2.at[dz, 0], (at(dz, 0), t))
        )
    for dp in range(1, q):
        first[dp - 1].wait_recv()
        got = full.at[:, :, col(at(0, q - dp))]
        for dz in range(1, q):
            second.append(push(got, got, s2.at[dz, dp], r2.at[dz, dp], (at(dz, 0), t)))
    own.wait()
    for copy in first:
        copy.wait_send()
    for copy in second:
        copy.wait()


def spread(n, q, nh):
    dma = pltpu.SemaphoreType.DMA
    return pl.pallas_call(
        functools.partial(spread_kernel, q),
        out_shape=jax.ShapeDtypeStruct((q, nh.shape[2], n * LANES), BF16),
        in_specs=[VMEM_SPEC],
        out_specs=VMEM_SPEC,
        scratch_shapes=[dma((q,)), dma((q,)), dma((q, q)), dma((q, q)), dma((1,))],
        compiler_params=pltpu.CompilerParams(collective_id=1, has_side_effects=True),
        name="spread",
    )(nh)


def settle_kernel(q, part, both, s1, r1, s2, r2, ls):
    s, t = lax.axis_index("sp"), lax.axis_index("tp")
    z, p = s // q, s % q
    wide = part.shape[2]

    def at(dz):
        return lax.rem(z + dz, q) * q + p

    def col(i):
        return pl.ds(pl.multiple_of(i * wide, wide), wide)

    greet([(at(d), t) for d in range(1, q)] + [(s, 1 - t)])
    first = []
    for dz in range(1, q):
        first.append(
            push(
                part.at[lax.rem(z + dz, q)], both.at[t, :, col(z)],
                s1.at[dz], r1.at[dz], (at(dz), t),
            )
        )
    own = pltpu.make_async_copy(part.at[z], both.at[t, :, col(z)], ls.at[0])
    own.start()
    second = [push(part.at[z], both.at[t, :, col(z)], s2.at[0], r2.at[0], (s, 1 - t))]
    for dz in range(1, q):
        first[dz - 1].wait_recv()
        got = both.at[t, :, col(lax.rem(z + q - dz, q))]
        second.append(push(got, got, s2.at[dz], r2.at[dz], (s, 1 - t)))
    own.wait()
    for copy in first:
        copy.wait_send()
    for copy in second:
        copy.wait()


def exchange(q, part):
    dma = pltpu.SemaphoreType.DMA
    return pl.pallas_call(
        functools.partial(settle_kernel, q),
        out_shape=jax.ShapeDtypeStruct((2, part.shape[1], q * part.shape[2]), BF16),
        in_specs=[VMEM_SPEC],
        out_specs=VMEM_SPEC,
        scratch_shapes=[dma((q,)), dma((q,)), dma((q,)), dma((q,)), dma((1,))],
        compiler_params=pltpu.CompilerParams(collective_id=2, has_side_effects=True),
        name="exchange",
    )(part)


def silu(x):
    return x * jax.nn.sigmoid(x)


def mix_kernel(tok, wts, taps, offsets, rates, gain, out, raw, gate, pre, vals, keys, reads, cums, yy, injf, injb):
    seq = tok.shape[0]
    rows = 2 * BLOCK
    wide = 3 * LANES
    blocks = seq // BLOCK
    raw[0:8, :] = jnp.zeros((8, wide), F32)
    raw[seq + 8 : seq + 16, :] = jnp.zeros((8, wide), F32)

    @pl.loop(0, seq // rows)
    def _(i):
        r0 = pl.multiple_of(i * rows, rows)
        got = jnp.dot(tok[pl.ds(r0, rows), :], wts[...], preferred_element_type=F32).astype(BF16)
        for a, b in ((0, 0), (2, 1), (3, 2)):
            raw[pl.ds(r0 + 8, rows), b * LANES : (b + 1) * LANES] = got[
                :, a * LANES : (a + 1) * LANES
            ].astype(F32)
        gate[pl.ds(r0, rows), :] = got[:, LANES : 2 * LANES]
        x = got[:, 4 * LANES :].astype(F32) + offsets[...]
        pre[pl.ds(r0, rows), :] = jnp.maximum(x, 0.0) + jnp.log1p(jnp.exp(-jnp.abs(x)))

    @pl.loop(0, blocks)
    def _(i):
        r0 = pl.multiple_of(i * BLOCK, BLOCK)
        for b, dst in enumerate((vals, keys, reads)):
            window = raw[pl.ds(r0, BLOCK + 16), b * LANES : (b + 1) * LANES]
            total = jnp.zeros((BLOCK, LANES), F32)
            for k in range(KERNEL):
                lo = 8 - (KERNEL - 1) // 2 + k
                total = total + window[lo : lo + BLOCK] * taps[k : k + 1, b * LANES : (b + 1) * LANES]
            dst[pl.ds(r0, BLOCK), :] = silu(total).astype(BF16)

    ri = lax.broadcasted_iota(jnp.int32, (BLOCK, BLOCK), 0)
    ci = lax.broadcasted_iota(jnp.int32, (BLOCK, BLOCK), 1)
    low = ri >= ci
    diag = ri == ci
    fwd = ci < 2
    left = ci < HEAD_DIM
    lower = jnp.where(low, 1.0, 0.0).astype(F32)
    upper = jnp.where(ri <= ci, 1.0, 0.0).astype(F32)

    @pl.loop(0, blocks)
    def _(i):
        r0 = pl.multiple_of(i * BLOCK, BLOCK)
        at = pl.ds(r0, BLOCK)
        st = pre[at, :]
        ld = -rates[...] * st
        c = jnp.where(
            fwd,
            jnp.dot(lower, ld, precision=FULL_PRECISION, preferred_element_type=F32),
            jnp.dot(upper, ld, precision=FULL_PRECISION, preferred_element_type=F32),
        )
        cums[at, :] = c
        ct = c.T
        stt = st.T
        key, read, val = keys[at, :], reads[at, :], vals[at, :]
        val32 = val.astype(F32)
        score = lax.dot_general(read, key, (((1,), (1,)), ((), ())), preferred_element_type=F32)
        total = jnp.zeros((BLOCK, LANES), F32)
        for h in range(2):
            gap = jnp.where(low, c[:, h : h + 1] - ct[h : h + 1, :], c[:, h + 2 : h + 3] - ct[h + 2 : h + 3, :])
            sb = stt[h + 2 : h + 3, :]
            e = jnp.exp(gap) * jnp.where(low, stt[h : h + 1, :], sb) + jnp.where(diag, sb, 0.0)
            side = left if h == 0 else jnp.logical_not(left)
            own = jnp.where(side, val32, 0.0).astype(BF16)
            total = total + jnp.dot((score * e).astype(BF16), own, preferred_element_type=F32)
        yy[at, :] = total
        c_end = jnp.where(fwd[0:1], c[BLOCK - 1 : BLOCK, :], c[0:1, :])
        weighting = jnp.exp(c_end - c) * st
        key_t = key.astype(F32).T.astype(BF16)
        for d, dst in ((0, injf), (1, injb)):
            w = jnp.where(left, weighting[:, 2 * d : 2 * d + 1], weighting[:, 2 * d + 1 : 2 * d + 2])
            scaled = (val32 * w).astype(BF16)
            dst[i] = jnp.dot(key_t, scaled, preferred_element_type=F32)

    def carry(i, state, d, inj):
        r0 = pl.multiple_of(i * BLOCK, BLOCK)
        at = pl.ds(r0, BLOCK)
        ec = jnp.exp(cums[at, :])
        grown = jnp.where(left, ec[:, 2 * d : 2 * d + 1], ec[:, 2 * d + 1 : 2 * d + 2])
        high = state.astype(BF16)
        rest = (state - high.astype(F32)).astype(BF16)
        read = reads[at, :]
        add = jnp.dot(read, high, preferred_element_type=F32) + jnp.dot(
            read, rest, preferred_element_type=F32
        )
        yy[at, :] = yy[at, :] + add * grown
        end = grown[BLOCK - 1 : BLOCK, :] if d == 0 else grown[0:1, :]
        return state * end + inj[i]

    def both(i, states):
        return (
            carry(i, states[0], 0, injf),
            carry(blocks - 1 - i, states[1], 1, injb),
        )

    zero = jnp.zeros((STATE, LANES), F32)
    lax.fori_loop(0, blocks, both, (zero, zero))

    @pl.loop(0, blocks)
    def _(i):
        r0 = pl.multiple_of(i * BLOCK, BLOCK)
        at = pl.ds(r0, BLOCK)
        g = yy[at, :] * silu(gate[at, :].astype(F32))
        sq = g * g
        m0 = jnp.sum(jnp.where(left, sq, 0.0), -1, keepdims=True) / HEAD_DIM
        m1 = jnp.sum(jnp.where(left, 0.0, sq), -1, keepdims=True) / HEAD_DIM
        scale = jnp.where(left, lax.rsqrt(m0 + EPSILON), lax.rsqrt(m1 + EPSILON))
        out[at, :] = (g * scale * gain[...]).astype(BF16)


def mix(tok, wts, taps, offsets, rates, gain):
    seq = tok.shape[0]
    vm = pltpu.VMEM
    return pl.pallas_call(
        mix_kernel,
        out_shape=jax.ShapeDtypeStruct((seq, LANES), BF16),
        in_specs=[VMEM_SPEC] * 6,
        out_specs=VMEM_SPEC,
        scratch_shapes=[
            vm((seq + 16, 3 * LANES), F32),
            vm((seq, LANES), BF16),
            vm((seq, LANES), F32),
            vm((seq, LANES), BF16),
            vm((seq, LANES), BF16),
            vm((seq, LANES), BF16),
            vm((seq, LANES), F32),
            vm((seq, LANES), F32),
            vm((seq // BLOCK, STATE, LANES), F32),
            vm((seq // BLOCK, STATE, LANES), F32),
        ],
        compiler_params=pltpu.CompilerParams(vmem_limit_bytes=48 << 20),
        name="mix",
    )(tok, wts, taps, offsets, rates, gain)


def own_lanes(fwd, bwd, n):
    both = jnp.stack([fwd.reshape(fwd.shape[0], n, -1), bwd.reshape(bwd.shape[0], n, -1)], 2)
    both = both.reshape(fwd.shape[0], n, -1)
    both = jnp.pad(both, ((0, 0), (0, 0), (0, LANES - both.shape[2])))
    return both.transpose(1, 0, 2)


def headwise(
    n,
    q,
    tokens,
    in_gain,
    w_value,
    w_gate,
    w_in_key,
    w_read,
    w_step_fwd,
    w_step_bwd,
    conv_value,
    conv_key,
    conv_read,
    step_bias,
    rate,
    norm_gain,
    w_out,
):
    s = lax.axis_index("sp")
    group = s // (n // (w_in_key.shape[1] // LANES))
    nrm = normalize(tokens.astype(F32), in_gain.astype(F32)).astype(BF16)
    steps = own_lanes(w_step_fwd, w_step_bwd, n)
    tok, wts, wout = gather(n, q, nrm, w_value, w_gate, w_in_key, w_read, steps, w_out)
    seq = n * nrm.shape[0]

    def cut(x, j):
        return lax.dynamic_slice_in_dim(x, j * LANES, LANES, 1)

    taps = jnp.concatenate([cut(conv_value, s), cut(conv_key, group), cut(conv_read, group)], 1)
    small = own_lanes(
        jnp.stack([step_bias[0], rate[0]]), jnp.stack([step_bias[1], rate[1]]), n
    )
    small = lax.dynamic_index_in_dim(small, s, 0, keepdims=False)
    gain = lax.dynamic_slice_in_dim(norm_gain, s * LANES, LANES, 0).astype(F32)[None]
    nh = mix(
        tok.reshape(seq, nrm.shape[1]), wts, taps.astype(F32), small[0:1], small[1:2], gain
    )
    full = spread(n, q, nh.reshape(q, q, nrm.shape[0], LANES))
    part = jnp.einsum("zrk,kc->zrc", full, wout, preferred_element_type=F32).astype(BF16)
    halves = exchange(q, part)
    return (halves[0].astype(F32) + halves[1].astype(F32)).astype(BF16)


def whole_heads(mesh):
    n, q = mesh.shape["sp"], math.isqrt(mesh.shape["sp"])

    def run(*args):
        cols, keys = args[2].shape[1], args[4].shape[1]
        ready = (
            q * q == n
            and mesh.shape["tp"] == 2
            and cols == n * LANES
            and args[14].shape[1] == LANES
            and keys % LANES == 0
            and n % (keys // LANES) == 0
            and args[0].shape[0] == BLOCK
        )
        return headwise(n, q, *args) if ready else body(*args)

    return run


def solution(mesh):
    in_specs = (
        P("sp", None),
        P(),
        P("sp", "tp"),
        P("sp", "tp"),
        P("sp", "tp"),
        P("sp", "tp"),
        P("sp", "tp"),
        P("sp", "tp"),
        P(None, "tp"),
        P(None, "tp"),
        P(None, "tp"),
        P(None, "tp"),
        P(None, "tp"),
        P("tp"),
        P("tp", "sp"),
    )
    out_specs = P("sp", None)
    return jax.shard_map(whole_heads(mesh), mesh=mesh, in_specs=in_specs, out_specs=out_specs, check_vma=False)
```

```python
import functools
import math

import jax
import jax.numpy as jnp
from jax import lax
from jax.experimental import pallas as pl
from jax.experimental.pallas import tpu as pltpu
from jax.sharding import PartitionSpec as P

HEAD_DIM = 64
STATE = 128
KERNEL = 5
BLOCK = 128


EPSILON = 1e-05
FULL_PRECISION = lax.Precision.HIGHEST


def entering_2(x, axis, combine, identity, reverse):
    length, place = (lax.axis_size(axis), lax.axis_index(axis))
    everything = jax.tree.map(lambda part: lax.all_gather(part, axis), x)
    start = jax.tree.map(
        lambda part, zero: jnp.broadcast_to(jnp.asarray(zero, part.dtype), part.shape), x, identity
    )

    def step(k, before):
        at = length - 1 - k if reverse else k
        reached = at > place if reverse else at < place
        new = combine(before, jax.tree.map(lambda part: part[at], everything))
        return jax.tree.map(lambda a, b: jnp.where(reached, a, b), new, before)

    return lax.fori_loop(0, length, step, start)


def with_halo(cells, sides, width):
    for axis, dim in sides:
        count = lax.axis_size(axis)
        ends = count - 1
        head = lax.slice_in_dim(cells, 0, width, axis=dim)
        tail = lax.slice_in_dim(cells, cells.shape[dim] - width, cells.shape[dim], axis=dim)
        cells = jnp.concatenate(
            [
                lax.ppermute(tail, axis, [(i, (i + 1) % count) for i in range(ends)]),
                cells,
                lax.ppermute(head, axis, [((i + 1) % count, i) for i in range(ends)]),
            ],
            axis=dim,
        )
    return cells


def normalize(tensor, gain):
    return tensor * lax.rsqrt(jnp.mean(tensor * tensor, -1, keepdims=True) + EPSILON) * gain


def block_parts(values, step_size, log_decay, in_keys):
    per_group = values.shape[1] // in_keys.shape[1]
    cumulative = jnp.cumsum(log_decay, axis=0)
    log_total = cumulative[-1]
    weighting = jnp.exp(log_total[None, :] - cumulative) * step_size
    key_heads = jnp.repeat(in_keys, per_group, axis=1)
    scaled = (values.astype(jnp.float32) * weighting[:, :, None]).astype(jnp.bfloat16)
    injected = jnp.einsum("jhn,jhp->hpn", key_heads, scaled, preferred_element_type=jnp.float32)
    return (cumulative, jnp.exp(log_total), injected)


def block_step(memory, inputs):
    values, step_size, cumulative, damping, injected, in_keys, read_in = inputs
    per_group = values.shape[1] // in_keys.shape[1]
    scores = jnp.einsum("ign,jgn->ijg", read_in, in_keys, preferred_element_type=jnp.float32)
    scores = jnp.repeat(scores, per_group, axis=2)
    length = values.shape[0]
    below_mask = (jnp.arange(length)[:, None] >= jnp.arange(length)[None, :])[:, :, None]
    gaps = jnp.where(below_mask, cumulative[:, None, :] - cumulative[None, :, :], -jnp.inf)
    weights = (scores * jnp.exp(gaps) * step_size[None, :, :]).astype(jnp.bfloat16)
    within = jnp.einsum("ijh,jhp->ihp", weights, values, preferred_element_type=jnp.float32)
    read_heads = jnp.repeat(read_in.astype(jnp.float32), per_group, axis=1)
    carried = (
        jnp.einsum("ihn,hpn->ihp", read_heads, memory, precision=FULL_PRECISION)
        * jnp.exp(cumulative)[:, :, None]
    )
    memory = damping[:, None, None] * memory + injected
    return (memory, within + carried)


def blocked(tensor):
    blocks = tensor.shape[0] // BLOCK
    return tensor.reshape((blocks, BLOCK) + tensor.shape[1:])


def sweep(block_inputs, memory):
    memory, swept = lax.scan(block_step, memory, block_inputs)
    return (swept.reshape((swept.shape[0] * swept.shape[1],) + swept.shape[2:]), memory)


def settle(damping_blocks, injected_blocks, memory):

    def advance(memory, inputs):
        return (inputs[0][:, None, None] * memory + inputs[1], None)

    memory, unused = lax.scan(advance, memory, (damping_blocks, injected_blocks))
    return memory


def chain(before_pair, after_pair):
    return (
        before_pair[0] * after_pair[0],
        after_pair[0][:, None, None] * before_pair[1] + after_pair[1],
    )


def entering(damping, final_state, backward):
    identity_pair = (jnp.ones_like(damping), jnp.zeros_like(final_state))
    if backward:
        arrived = entering_2((damping, final_state), "sp", chain, identity_pair, True)
    else:
        arrived = entering_2((damping, final_state), "sp", chain, identity_pair, False)
    return arrived[1]


def body(
    tokens,
    in_gain,
    w_value,
    w_gate,
    w_in_key,
    w_read,
    w_step_fwd,
    w_step_bwd,
    conv_value,
    conv_key,
    conv_read,
    step_bias,
    rate,
    norm_gain,
    w_out,
):
    normed = normalize(tokens.astype(jnp.float32), in_gain.astype(jnp.float32)).astype(jnp.bfloat16)
    weights = (
        lax.all_gather(w_value, "sp", axis=0, tiled=True),
        lax.all_gather(w_gate, "sp", axis=0, tiled=True),
        lax.all_gather(w_in_key, "sp", axis=0, tiled=True),
        lax.all_gather(w_read, "sp", axis=0, tiled=True),
        lax.all_gather(w_step_fwd, "sp", axis=0, tiled=True),
        lax.all_gather(w_step_bwd, "sp", axis=0, tiled=True),
    )
    projected = [
        jnp.dot(normed, weight, preferred_element_type=jnp.float32).astype(jnp.bfloat16)
        for weight in weights
    ]
    value_raw, gate_raw, key_raw, read_raw, pre_fwd, pre_bwd = projected
    value_cols = value_raw.shape[1]
    key_cols = key_raw.shape[1]
    joined = jnp.concatenate([value_raw, key_raw, read_raw], axis=1)
    padded = with_halo(joined, (("sp", 0),), (KERNEL - 1) // 2)
    kernel_taps = jnp.concatenate([conv_value, conv_key, conv_read], axis=1).astype(jnp.float32)
    length = joined.shape[0]
    summed = jnp.zeros(joined.shape, jnp.float32)
    for offset in range(KERNEL):
        summed = summed + padded[offset : offset + length].astype(jnp.float32) * kernel_taps[offset]
    mixed_in = jax.nn.silu(summed).astype(jnp.bfloat16)
    head_count = value_cols // HEAD_DIM
    group_count = key_cols // STATE
    values = mixed_in[:, :value_cols].reshape(length, head_count, HEAD_DIM)
    in_keys = mixed_in[:, value_cols : value_cols + key_cols].reshape(length, group_count, STATE)
    read_in = mixed_in[:, value_cols + key_cols :].reshape(length, group_count, STATE)
    blank = jnp.zeros((head_count, HEAD_DIM, STATE), jnp.float32)
    summed_heads = jnp.zeros(values.shape, jnp.float32)
    for direction, step_pre in ((0, pre_fwd), (1, pre_bwd)):
        step_size = jax.nn.softplus(step_pre.astype(jnp.float32) + step_bias[direction])
        log_decay = -rate[direction] * step_size
        ordered = (values, step_size, log_decay, in_keys, read_in)
        if direction == 1:
            ordered = tuple((tensor[::-1] for tensor in ordered))
        value_blocks, step_blocks, decay_blocks, key_blocks, read_blocks = [
            blocked(tensor) for tensor in ordered
        ]
        cumulative_blocks, damping_blocks, injected_blocks = jax.vmap(block_parts)(
            value_blocks, step_blocks, decay_blocks, key_blocks
        )
        block_inputs = (
            value_blocks,
            step_blocks,
            cumulative_blocks,
            damping_blocks,
            injected_blocks,
            key_blocks,
            read_blocks,
        )
        damping = jnp.exp(jnp.sum(ordered[2], axis=0))
        final_state = settle(damping_blocks, injected_blocks, blank)
        arriving = entering(damping, final_state, direction == 1)
        swept, final_state = sweep(block_inputs, arriving)
        if direction == 1:
            swept = swept[::-1]
        summed_heads = summed_heads + swept
    gated_out = summed_heads * jax.nn.silu(gate_raw.astype(jnp.float32)).reshape(values.shape)
    head_gain = norm_gain.astype(jnp.float32).reshape(head_count, HEAD_DIM)
    normed_heads = normalize(gated_out, head_gain).astype(jnp.bfloat16).reshape(length, value_cols)
    out_whole = lax.all_gather(w_out, "sp", axis=1, tiled=True)
    own_rows = lax.psum_scatter(
        jnp.dot(normed_heads, out_whole, preferred_element_type=jnp.float32).astype(jnp.bfloat16),
        "tp",
        scatter_dimension=0,
        tiled=True,
    )
    return lax.all_gather(own_rows, "tp", axis=0, tiled=True)


F32 = jnp.float32
BF16 = jnp.bfloat16
LANES = 128
VMEM_SPEC = pl.BlockSpec(memory_space=pltpu.VMEM)


def greet(peers):
    barrier = pltpu.get_barrier_semaphore()
    for peer in peers:
        pl.semaphore_signal(
            barrier, inc=1, device_id=peer, device_id_type=pl.DeviceIdType.MESH
        )
    pl.semaphore_wait(barrier, len(peers))


def push(src, dst, send, recv, peer):
    copy = pltpu.make_async_remote_copy(
        src_ref=src,
        dst_ref=dst,
        send_sem=send,
        recv_sem=recv,
        device_id=peer,
        device_id_type=pl.DeviceIdType.MESH,
    )
    copy.start()
    return copy


def silu(x):
    return x * jax.nn.sigmoid(x)


def whole_kernel(
    n, q, nrm, wv, wg, wk, wr, ws, wo, taps, offsets, rates, gain, both,
    tok, wts, wst, wout, raw, gate, pre, vals, keys, reads, cums, yy, injf, injb, nh, full, part,
    tzs, tzr, tps, tpr, tss, tsr, kzs, kzr, kps, kpr, vs, vr, ss, sr, os, orr,
    as_, ar, bs, br, es, er, fs, fr, ls,
):
    s, t = lax.axis_index("sp"), lax.axis_index("tp")
    z, p = s // q, s % q
    sibling = (s, 1 - t)
    half = tok.shape[2]
    depth = wv.shape[0]
    blocks = tok.shape[0] * 2 * half // BLOCK

    def at(dz, dp):
        return lax.rem(z + dz, q) * q + lax.rem(p + dp, q)

    def span(i, size):
        return pl.ds(pl.multiple_of(i * size, size), size)

    greet([(lax.rem(s + k, n), t) for k in range(1, n)] + [sibling])
    done, sent = [], []

    def local(src, dst, i):
        copy = pltpu.make_async_copy(src, dst, ls.at[i])
        copy.start()
        return copy

    mine = span(s, depth)
    rows = span(t, half)
    kcol, rcol = pl.ds(2 * LANES, LANES), pl.ds(3 * LANES, LANES)
    first, keyz = [], []
    for dz in range(1, q):
        first.append(push(nrm.at[rows], tok.at[s, t], tzs.at[dz], tzr.at[dz], (at(dz, 0), t)))
    for dz in range(1, q):
        grp = span(lax.rem(z + dz, q), LANES)
        keyz.append(
            [
                push(w.at[:, grp], wts.at[mine, col], kzs.at[dz, i], kzr.at[dz, i], (at(dz, 0), t))
                for i, (w, col) in enumerate(((wk, kcol), (wr, rcol)))
            ]
        )
    plane, keyp = {}, []
    for dp in range(1, q):
        plane[0, dp] = push(nrm.at[rows], tok.at[s, t], tps.at[0, dp], tpr.at[0, dp], (at(0, dp), t))
    for dp in range(1, q):
        for i, (w, col) in enumerate(((wk, kcol), (wr, rcol))):
            keyp.append(
                push(
                    w.at[:, span(z, LANES)], wts.at[mine, col],
                    kps.at[i * q, dp], kpr.at[i * q, dp], (at(0, dp), t),
                )
            )
    locals_ = [
        local(nrm.at[pl.ds(0, half)], tok.at[s, 0], 0),
        local(nrm.at[pl.ds(half, half)], tok.at[s, 1], 1),
        local(wk.at[:, span(z, LANES)], wts.at[mine, kcol], 2),
        local(wr.at[:, span(z, LANES)], wts.at[mine, rcol], 3),
        local(wv.at[:, mine], wts.at[mine, pl.ds(0, LANES)], 4),
        local(wg.at[:, mine], wts.at[mine, pl.ds(LANES, LANES)], 5),
        local(ws.at[s], wst.at[pl.ds(0, ws.shape[1]), mine], 6),
    ]
    weights = []
    for k in range(1, n):
        j = lax.rem(s + k, n)
        cols = span(j, LANES)
        for i, w in enumerate((wv, wg)):
            weights.append(
                push(w.at[:, cols], wts.at[mine, pl.ds(i * LANES, LANES)], vs.at[k, i], vr.at[k, i], (j, t))
            )
        weights.append(
            push(ws.at[j], wst.at[pl.ds(0, ws.shape[1]), mine], ss.at[k], sr.at[k], (j, t))
        )
    swaps = {}

    def swap(dz, dp):
        src = at(q - dz, q - dp)
        swaps[dz, dp] = push(tok.at[src, t], tok.at[src, t], tss.at[dz, dp], tsr.at[dz, dp], sibling)

    for dz in range(1, q):
        src = at(q - dz, 0)
        first[dz - 1].wait_recv()
        for dp in range(1, q):
            plane[dz, dp] = push(tok.at[src, t], tok.at[src, t], tps.at[dz, dp], tpr.at[dz, dp], (at(0, dp), t))
        swap(dz, 0)
        for copy in keyz[dz - 1]:
            copy.wait_recv()
        got = wts.at[span(src, depth), pl.ds(2 * LANES, 2 * LANES)]
        for dp in range(1, q):
            keyp.append(push(got, got, kps.at[dz, dp], kpr.at[dz, dp], (at(0, dp), t)))
    outs = []
    for dz in range(1, q):
        outs.append(push(wo, wout.at[:, span(z, LANES)], os.at[dz], orr.at[dz], (at(dz, 0), t)))
    locals_.append(local(wo, wout.at[:, span(z, LANES)], 7))

    wst[ws.shape[1] :, :] = jnp.zeros((LANES - ws.shape[1], wst.shape[1]), BF16)
    seq = blocks * BLOCK
    wide = 3 * LANES
    raw[0:8, :] = jnp.zeros((8, wide), F32)
    raw[seq + 8 : seq + 16, :] = jnp.zeros((8, wide), F32)
    for copy in locals_:
        copy.wait()
    for copy in weights + keyp:
        copy.wait_recv()

    def project(plane_index):
        @pl.loop(0, q // 2)
        def _(i):
            chip = plane_index * q + 2 * i
            r0 = pl.multiple_of(chip * BLOCK, 2 * BLOCK)
            at2 = pl.ds(r0, 2 * BLOCK)
            x = tok[pl.ds(chip, 2)].reshape(2 * BLOCK, tok.shape[3])
            got = jnp.dot(x, wts[...], preferred_element_type=F32).astype(BF16)
            for i_, b_ in ((0, 0), (2, 1), (3, 2)):
                raw[pl.ds(r0 + 8, 2 * BLOCK), b_ * LANES : (b_ + 1) * LANES] = got[
                    :, i_ * LANES : (i_ + 1) * LANES
                ].astype(F32)
            gate[at2, :] = got[:, LANES : 2 * LANES]
            u = lax.dot_general(x, wst[...], (((1,), (1,)), ((), ())), preferred_element_type=F32)
            u = u.astype(BF16).astype(F32) + offsets[...]
            pre[at2, :] = jnp.maximum(u, 0.0) + jnp.log1p(jnp.exp(-jnp.abs(u)))

    for dz in range(q):
        for dp in range(1, q):
            plane[dz, dp].wait_recv()
            swap(dz, dp)
        for dp in range(q):
            if (dz, dp) != (0, 0):
                swaps[dz, dp].wait_recv()
        project(lax.rem(z + q - dz, q))

    @pl.loop(0, blocks)
    def _(i):
        r0 = pl.multiple_of(i * BLOCK, BLOCK)
        for b, dst in enumerate((vals, keys, reads)):
            window = raw[pl.ds(r0, BLOCK + 16), b * LANES : (b + 1) * LANES]
            total = jnp.zeros((BLOCK, LANES), F32)
            for k in range(KERNEL):
                lo = 8 - (KERNEL - 1) // 2 + k
                total = total + window[lo : lo + BLOCK] * taps[k : k + 1, b * LANES : (b + 1) * LANES]
            dst[pl.ds(r0, BLOCK), :] = silu(total).astype(BF16)

    ri = lax.broadcasted_iota(jnp.int32, (BLOCK, BLOCK), 0)
    ci = lax.broadcasted_iota(jnp.int32, (BLOCK, BLOCK), 1)
    low = ri >= ci
    diag = ri == ci
    fwd = ci < 2
    left = ci < HEAD_DIM
    lower = jnp.where(low, 1.0, 0.0).astype(F32)
    upper = jnp.where(ri <= ci, 1.0, 0.0).astype(F32)

    @pl.loop(0, blocks)
    def _(i):
        r0 = pl.multiple_of(i * BLOCK, BLOCK)
        here = pl.ds(r0, BLOCK)
        st = pre[here, :]
        ld = -rates[...] * st
        c = jnp.where(
            fwd,
            jnp.dot(lower, ld, precision=FULL_PRECISION, preferred_element_type=F32),
            jnp.dot(upper, ld, precision=FULL_PRECISION, preferred_element_type=F32),
        )
        cums[here, :] = c
        ct = c.T
        stt = st.T
        key, read, val = keys[here, :], reads[here, :], vals[here, :]
        val32 = val.astype(F32)
        score = lax.dot_general(read, key, (((1,), (1,)), ((), ())), preferred_element_type=F32)
        total = jnp.zeros((BLOCK, LANES), F32)
        for h in range(2):
            gap = jnp.where(low, c[:, h : h + 1] - ct[h : h + 1, :], c[:, h + 2 : h + 3] - ct[h + 2 : h + 3, :])
            sb = stt[h + 2 : h + 3, :]
            e = jnp.exp(gap) * jnp.where(low, stt[h : h + 1, :], sb) + jnp.where(diag, sb, 0.0)
            side = left if h == 0 else jnp.logical_not(left)
            own = jnp.where(side, val32, 0.0).astype(BF16)
            total = total + jnp.dot((score * e).astype(BF16), own, preferred_element_type=F32)
        yy[here, :] = total
        c_end = jnp.where(fwd[0:1], c[BLOCK - 1 : BLOCK, :], c[0:1, :])
        weighting = jnp.exp(c_end - c) * st
        key_t = key.astype(F32).T.astype(BF16)
        for d, dst in ((0, injf), (1, injb)):
            w = jnp.where(left, weighting[:, 2 * d : 2 * d + 1], weighting[:, 2 * d + 1 : 2 * d + 2])
            scaled = (val32 * w).astype(BF16)
            dst[i] = jnp.dot(key_t, scaled, preferred_element_type=F32)

    def carry(i, state, d, inj):
        r0 = pl.multiple_of(i * BLOCK, BLOCK)
        here = pl.ds(r0, BLOCK)
        ec = jnp.exp(cums[here, :])
        grown = jnp.where(left, ec[:, 2 * d : 2 * d + 1], ec[:, 2 * d + 1 : 2 * d + 2])
        high = state.astype(BF16)
        rest = (state - high.astype(F32)).astype(BF16)
        read = reads[here, :]
        add = jnp.dot(read, high, preferred_element_type=F32) + jnp.dot(
            read, rest, preferred_element_type=F32
        )
        yy[here, :] = yy[here, :] + add * grown
        end = grown[BLOCK - 1 : BLOCK, :] if d == 0 else grown[0:1, :]
        return state * end + inj[i]

    def advance(i, states):
        return (
            carry(i, states[0], 0, injf),
            carry(blocks - 1 - i, states[1], 1, injb),
        )

    zero = jnp.zeros((STATE, LANES), F32)
    lax.fori_loop(0, blocks, advance, (zero, zero))

    def finish(i):
        r0 = pl.multiple_of(i * BLOCK, BLOCK)
        here = pl.ds(r0, BLOCK)
        g = yy[here, :] * silu(gate[here, :].astype(F32))
        sq = g * g
        m0 = jnp.sum(jnp.where(left, sq, 0.0), -1, keepdims=True) / HEAD_DIM
        m1 = jnp.sum(jnp.where(left, 0.0, sq), -1, keepdims=True) / HEAD_DIM
        scale = jnp.where(left, lax.rsqrt(m0 + EPSILON), lax.rsqrt(m1 + EPSILON))
        nh[here, :] = (g * scale * gain[...]).astype(BF16)

    away = []
    for dz in range(1, q + 1):
        to = lax.rem(z + dz, q)

        @pl.loop(0, q)
        def _(i):
            finish(to * q + i)

        if dz < q:
            away.append(
                push(nh.at[span(to, q * BLOCK)], full.at[:, mine], as_.at[dz], ar.at[dz], (at(dz, 0), t))
            )
    near = {}
    keep = local(nh.at[span(z, q * BLOCK)], full.at[:, mine], 8)
    for dp in range(1, q):
        near[0, dp] = push(
            nh.at[span(z, q * BLOCK)], full.at[:, mine], bs.at[0, dp], br.at[0, dp], (at(0, dp), t)
        )
    for dz in range(1, q):
        away[dz - 1].wait_recv()
        got = full.at[:, span(at(q - dz, 0), LANES)]
        for dp in range(1, q):
            near[dz, dp] = push(got, got, bs.at[dz, dp], br.at[dz, dp], (at(0, dp), t))
    keep.wait()
    for copy in outs + list(near.values()):
        copy.wait_recv()
    legs = []
    for dp in range(1, q + 1):
        to = lax.rem(p + dp, q)
        part[to] = jnp.dot(full[span(to, BLOCK), :], wout[...], preferred_element_type=F32).astype(BF16)
    for dp in range(1, q):
        to = lax.rem(p + dp, q)
        legs.append(push(part.at[to], both.at[t, p], es.at[dp], er.at[dp], (at(0, dp), t)))
    across = [push(part.at[p], both.at[t, p], fs.at[0], fr.at[0], sibling)]
    keep = local(part.at[p], both.at[t, p], 9)
    for dp in range(1, q):
        legs[dp - 1].wait_recv()
        got = both.at[t, lax.rem(p + q - dp, q)]
        across.append(push(got, got, fs.at[dp], fr.at[dp], sibling))
    keep.wait()
    for copy in across:
        copy.wait()
    flat = [copy for pair in keyz for copy in pair]
    for copy in first + flat + list(plane.values()) + keyp + weights + list(swaps.values()):
        copy.wait_send()
    for copy in outs + away + list(near.values()) + legs:
        copy.wait_send()


def whole(n, q, nrm, wv, wg, wk, wr, ws, wo, taps, offsets, rates, gain):
    dma = pltpu.SemaphoreType.DMA
    vm = pltpu.VMEM
    depth = nrm.shape[0]
    width = nrm.shape[1]
    seq = n * depth
    return pl.pallas_call(
        functools.partial(whole_kernel, n, q),
        out_shape=jax.ShapeDtypeStruct((2, q, BLOCK, q * LANES), BF16),
        in_specs=[VMEM_SPEC] * 11,
        out_specs=VMEM_SPEC,
        scratch_shapes=[
            vm((n, 2, depth // 2, width), BF16),
            vm((width, 4 * LANES), BF16),
            vm((LANES, width), BF16),
            vm((wo.shape[0], q * LANES), BF16),
            vm((seq + 16, 3 * LANES), F32),
            vm((seq, LANES), BF16),
            vm((seq, LANES), F32),
            vm((seq, LANES), BF16),
            vm((seq, LANES), BF16),
            vm((seq, LANES), BF16),
            vm((seq, LANES), F32),
            vm((seq, LANES), F32),
            vm((seq // BLOCK, STATE, LANES), F32),
            vm((seq // BLOCK, STATE, LANES), F32),
            vm((seq, LANES), BF16),
            vm((q * BLOCK, n * LANES), BF16),
            vm((q, BLOCK, q * LANES), BF16),
            dma((q,)), dma((q,)), dma((q, q)), dma((q, q)), dma((q, q)), dma((q, q)),
            dma((q, 2)), dma((q, 2)), dma((q + 1, q)), dma((q + 1, q)),
            dma((n, 2)), dma((n, 2)), dma((n,)), dma((n,)), dma((q,)), dma((q,)),
            dma((q,)), dma((q,)), dma((q, q)), dma((q, q)), dma((q,)), dma((q,)),
            dma((q,)), dma((q,)), dma((10,)),
        ],
        compiler_params=pltpu.CompilerParams(
            collective_id=0, has_side_effects=True, vmem_limit_bytes=56 << 20
        ),
        name="whole",
    )(nrm, wv, wg, wk, wr, ws, wo, taps, offsets, rates, gain)


def own_lanes(fwd, bwd, n):
    both = jnp.stack([fwd.reshape(fwd.shape[0], n, -1), bwd.reshape(bwd.shape[0], n, -1)], 2)
    both = both.reshape(fwd.shape[0], n, -1)
    both = jnp.pad(both, ((0, 0), (0, 0), (0, LANES - both.shape[2])))
    return both.transpose(1, 0, 2)


def headwise(
    n,
    q,
    tokens,
    in_gain,
    w_value,
    w_gate,
    w_in_key,
    w_read,
    w_step_fwd,
    w_step_bwd,
    conv_value,
    conv_key,
    conv_read,
    step_bias,
    rate,
    norm_gain,
    w_out,
):
    s = lax.axis_index("sp")
    group = s // q
    nrm = normalize(tokens.astype(F32), in_gain.astype(F32)).astype(BF16)
    steps = own_lanes(w_step_fwd, w_step_bwd, n)[:, :, :16].transpose(0, 2, 1)

    def cut(x, j):
        return lax.dynamic_slice_in_dim(x, j * LANES, LANES, 1)

    taps = jnp.concatenate([cut(conv_value, s), cut(conv_key, group), cut(conv_read, group)], 1)
    small = own_lanes(
        jnp.stack([step_bias[0], rate[0]]), jnp.stack([step_bias[1], rate[1]]), n
    )
    small = lax.dynamic_index_in_dim(small, s, 0, keepdims=False)
    gain = lax.dynamic_slice_in_dim(norm_gain, s * LANES, LANES, 0).astype(F32)[None]
    halves = whole(
        n, q, nrm, w_value, w_gate, w_in_key, w_read, steps, w_out,
        taps.astype(F32), small[0:1], small[1:2], gain,
    )
    total = (halves[0].astype(F32) + halves[1].astype(F32)).astype(BF16)
    return total.reshape(q, BLOCK, q, LANES).transpose(1, 2, 0, 3).reshape(BLOCK, n * LANES)


def whole_heads(mesh):
    n, q = mesh.shape["sp"], math.isqrt(mesh.shape["sp"])

    def run(*args):
        cols, keys = args[2].shape[1], args[4].shape[1]
        ready = (
            q * q == n
            and mesh.shape["tp"] == 2
            and cols == n * LANES
            and args[14].shape[1] == LANES
            and keys == q * LANES
            and q % 2 == 0
            and args[0].shape[1] == n * LANES
            and args[0].shape[0] == BLOCK
        )
        return headwise(n, q, *args) if ready else body(*args)

    return run


def solution(mesh):
    in_specs = (
        P("sp", None),
        P(),
        P("sp", "tp"),
        P("sp", "tp"),
        P("sp", "tp"),
        P("sp", "tp"),
        P("sp", "tp"),
        P("sp", "tp"),
        P(None, "tp"),
        P(None, "tp"),
        P(None, "tp"),
        P(None, "tp"),
        P(None, "tp"),
        P("tp"),
        P("tp", "sp"),
    )
    out_specs = P("sp", None)
    return jax.shard_map(whole_heads(mesh), mesh=mesh, in_specs=in_specs, out_specs=out_specs, check_vma=False)
```

```python
import functools
import math

import jax
import jax.numpy as jnp
from jax import lax
from jax.experimental import pallas as pl
from jax.experimental.pallas import tpu as pltpu
from jax.sharding import PartitionSpec as P

HEAD_DIM = 64
STATE = 128
KERNEL = 5
BLOCK = 128


EPSILON = 1e-05
FULL_PRECISION = lax.Precision.HIGHEST


def entering_2(x, axis, combine, identity, reverse):
    length, place = (lax.axis_size(axis), lax.axis_index(axis))
    everything = jax.tree.map(lambda part: lax.all_gather(part, axis), x)
    start = jax.tree.map(
        lambda part, zero: jnp.broadcast_to(jnp.asarray(zero, part.dtype), part.shape), x, identity
    )

    def step(k, before):
        at = length - 1 - k if reverse else k
        reached = at > place if reverse else at < place
        new = combine(before, jax.tree.map(lambda part: part[at], everything))
        return jax.tree.map(lambda a, b: jnp.where(reached, a, b), new, before)

    return lax.fori_loop(0, length, step, start)


def with_halo(cells, sides, width):
    for axis, dim in sides:
        count = lax.axis_size(axis)
        ends = count - 1
        head = lax.slice_in_dim(cells, 0, width, axis=dim)
        tail = lax.slice_in_dim(cells, cells.shape[dim] - width, cells.shape[dim], axis=dim)
        cells = jnp.concatenate(
            [
                lax.ppermute(tail, axis, [(i, (i + 1) % count) for i in range(ends)]),
                cells,
                lax.ppermute(head, axis, [((i + 1) % count, i) for i in range(ends)]),
            ],
            axis=dim,
        )
    return cells


def normalize(tensor, gain):
    return tensor * lax.rsqrt(jnp.mean(tensor * tensor, -1, keepdims=True) + EPSILON) * gain


def block_parts(values, step_size, log_decay, in_keys):
    per_group = values.shape[1] // in_keys.shape[1]
    cumulative = jnp.cumsum(log_decay, axis=0)
    log_total = cumulative[-1]
    weighting = jnp.exp(log_total[None, :] - cumulative) * step_size
    key_heads = jnp.repeat(in_keys, per_group, axis=1)
    scaled = (values.astype(jnp.float32) * weighting[:, :, None]).astype(jnp.bfloat16)
    injected = jnp.einsum("jhn,jhp->hpn", key_heads, scaled, preferred_element_type=jnp.float32)
    return (cumulative, jnp.exp(log_total), injected)


def block_step(memory, inputs):
    values, step_size, cumulative, damping, injected, in_keys, read_in = inputs
    per_group = values.shape[1] // in_keys.shape[1]
    scores = jnp.einsum("ign,jgn->ijg", read_in, in_keys, preferred_element_type=jnp.float32)
    scores = jnp.repeat(scores, per_group, axis=2)
    length = values.shape[0]
    below_mask = (jnp.arange(length)[:, None] >= jnp.arange(length)[None, :])[:, :, None]
    gaps = jnp.where(below_mask, cumulative[:, None, :] - cumulative[None, :, :], -jnp.inf)
    weights = (scores * jnp.exp(gaps) * step_size[None, :, :]).astype(jnp.bfloat16)
    within = jnp.einsum("ijh,jhp->ihp", weights, values, preferred_element_type=jnp.float32)
    read_heads = jnp.repeat(read_in.astype(jnp.float32), per_group, axis=1)
    carried = (
        jnp.einsum("ihn,hpn->ihp", read_heads, memory, precision=FULL_PRECISION)
        * jnp.exp(cumulative)[:, :, None]
    )
    memory = damping[:, None, None] * memory + injected
    return (memory, within + carried)


def blocked(tensor):
    blocks = tensor.shape[0] // BLOCK
    return tensor.reshape((blocks, BLOCK) + tensor.shape[1:])


def sweep(block_inputs, memory):
    memory, swept = lax.scan(block_step, memory, block_inputs)
    return (swept.reshape((swept.shape[0] * swept.shape[1],) + swept.shape[2:]), memory)


def settle(damping_blocks, injected_blocks, memory):

    def advance(memory, inputs):
        return (inputs[0][:, None, None] * memory + inputs[1], None)

    memory, unused = lax.scan(advance, memory, (damping_blocks, injected_blocks))
    return memory


def chain(before_pair, after_pair):
    return (
        before_pair[0] * after_pair[0],
        after_pair[0][:, None, None] * before_pair[1] + after_pair[1],
    )


def entering(damping, final_state, backward):
    identity_pair = (jnp.ones_like(damping), jnp.zeros_like(final_state))
    if backward:
        arrived = entering_2((damping, final_state), "sp", chain, identity_pair, True)
    else:
        arrived = entering_2((damping, final_state), "sp", chain, identity_pair, False)
    return arrived[1]


def body(
    tokens,
    in_gain,
    w_value,
    w_gate,
    w_in_key,
    w_read,
    w_step_fwd,
    w_step_bwd,
    conv_value,
    conv_key,
    conv_read,
    step_bias,
    rate,
    norm_gain,
    w_out,
):
    normed = normalize(tokens.astype(jnp.float32), in_gain.astype(jnp.float32)).astype(jnp.bfloat16)
    weights = (
        lax.all_gather(w_value, "sp", axis=0, tiled=True),
        lax.all_gather(w_gate, "sp", axis=0, tiled=True),
        lax.all_gather(w_in_key, "sp", axis=0, tiled=True),
        lax.all_gather(w_read, "sp", axis=0, tiled=True),
        lax.all_gather(w_step_fwd, "sp", axis=0, tiled=True),
        lax.all_gather(w_step_bwd, "sp", axis=0, tiled=True),
    )
    projected = [
        jnp.dot(normed, weight, preferred_element_type=jnp.float32).astype(jnp.bfloat16)
        for weight in weights
    ]
    value_raw, gate_raw, key_raw, read_raw, pre_fwd, pre_bwd = projected
    value_cols = value_raw.shape[1]
    key_cols = key_raw.shape[1]
    joined = jnp.concatenate([value_raw, key_raw, read_raw], axis=1)
    padded = with_halo(joined, (("sp", 0),), (KERNEL - 1) // 2)
    kernel_taps = jnp.concatenate([conv_value, conv_key, conv_read], axis=1).astype(jnp.float32)
    length = joined.shape[0]
    summed = jnp.zeros(joined.shape, jnp.float32)
    for offset in range(KERNEL):
        summed = summed + padded[offset : offset + length].astype(jnp.float32) * kernel_taps[offset]
    mixed_in = jax.nn.silu(summed).astype(jnp.bfloat16)
    head_count = value_cols // HEAD_DIM
    group_count = key_cols // STATE
    values = mixed_in[:, :value_cols].reshape(length, head_count, HEAD_DIM)
    in_keys = mixed_in[:, value_cols : value_cols + key_cols].reshape(length, group_count, STATE)
    read_in = mixed_in[:, value_cols + key_cols :].reshape(length, group_count, STATE)
    blank = jnp.zeros((head_count, HEAD_DIM, STATE), jnp.float32)
    summed_heads = jnp.zeros(values.shape, jnp.float32)
    for direction, step_pre in ((0, pre_fwd), (1, pre_bwd)):
        step_size = jax.nn.softplus(step_pre.astype(jnp.float32) + step_bias[direction])
        log_decay = -rate[direction] * step_size
        ordered = (values, step_size, log_decay, in_keys, read_in)
        if direction == 1:
            ordered = tuple((tensor[::-1] for tensor in ordered))
        value_blocks, step_blocks, decay_blocks, key_blocks, read_blocks = [
            blocked(tensor) for tensor in ordered
        ]
        cumulative_blocks, damping_blocks, injected_blocks = jax.vmap(block_parts)(
            value_blocks, step_blocks, decay_blocks, key_blocks
        )
        block_inputs = (
            value_blocks,
            step_blocks,
            cumulative_blocks,
            damping_blocks,
            injected_blocks,
            key_blocks,
            read_blocks,
        )
        damping = jnp.exp(jnp.sum(ordered[2], axis=0))
        final_state = settle(damping_blocks, injected_blocks, blank)
        arriving = entering(damping, final_state, direction == 1)
        swept, final_state = sweep(block_inputs, arriving)
        if direction == 1:
            swept = swept[::-1]
        summed_heads = summed_heads + swept
    gated_out = summed_heads * jax.nn.silu(gate_raw.astype(jnp.float32)).reshape(values.shape)
    head_gain = norm_gain.astype(jnp.float32).reshape(head_count, HEAD_DIM)
    normed_heads = normalize(gated_out, head_gain).astype(jnp.bfloat16).reshape(length, value_cols)
    out_whole = lax.all_gather(w_out, "sp", axis=1, tiled=True)
    own_rows = lax.psum_scatter(
        jnp.dot(normed_heads, out_whole, preferred_element_type=jnp.float32).astype(jnp.bfloat16),
        "tp",
        scatter_dimension=0,
        tiled=True,
    )
    return lax.all_gather(own_rows, "tp", axis=0, tiled=True)


F32 = jnp.float32
BF16 = jnp.bfloat16
LANES = 128
VMEM_SPEC = pl.BlockSpec(memory_space=pltpu.VMEM)


def greet(peers):
    barrier = pltpu.get_barrier_semaphore()
    for peer in peers:
        pl.semaphore_signal(
            barrier, inc=1, device_id=peer, device_id_type=pl.DeviceIdType.MESH
        )
    pl.semaphore_wait(barrier, len(peers))


def push(src, dst, send, recv, peer):
    copy = pltpu.make_async_remote_copy(
        src_ref=src,
        dst_ref=dst,
        send_sem=send,
        recv_sem=recv,
        device_id=peer,
        device_id_type=pl.DeviceIdType.MESH,
    )
    copy.start()
    return copy


def silu(x):
    return x * jax.nn.sigmoid(x)


def whole_kernel(
    n, q, nrm, wv, wg, wk, wr, ws, wo, taps, offsets, rates, gain, out,
    tok, wts, wst, wout, raw, gate, pre, vals, keys, reads, cums, yy, injf, injb, carf, carb, nh, full, part, both,
    tzs, tzr, tps, tpr, tss, tsr, kzs, kzr, kps, kpr, vs, vr, ss, sr, os, orr,
    as_, ar, bs, br, es, er, fs, fr, ls,
):
    s, t = lax.axis_index("sp"), lax.axis_index("tp")
    z, p = s // q, s % q
    sibling = (s, 1 - t)
    half = tok.shape[2]
    depth = wv.shape[0]
    blocks = tok.shape[0] * 2 * half // BLOCK

    def at(dz, dp):
        return lax.rem(z + dz, q) * q + lax.rem(p + dp, q)

    def span(i, size):
        return pl.ds(pl.multiple_of(i * size, size), size)

    greet([(lax.rem(s + k, n), t) for k in range(1, n)] + [sibling])
    done, sent = [], []

    def local(src, dst, i):
        copy = pltpu.make_async_copy(src, dst, ls.at[i])
        copy.start()
        return copy

    mine = span(s, depth)
    rows = span(t, half)
    kcol, rcol = pl.ds(2 * LANES, LANES), pl.ds(3 * LANES, LANES)
    first, keyz = [], []
    for dz in range(1, q):
        first.append(push(nrm.at[rows], tok.at[s, t], tzs.at[dz], tzr.at[dz], (at(dz, 0), t)))
    for dz in range(1, q):
        grp = span(lax.rem(z + dz, q), LANES)
        keyz.append(
            [
                push(w.at[:, grp], wts.at[mine, col], kzs.at[dz, i], kzr.at[dz, i], (at(dz, 0), t))
                for i, (w, col) in enumerate(((wk, kcol), (wr, rcol)))
            ]
        )
    plane, keyp = {}, []
    for dp in range(1, q):
        plane[0, dp] = push(nrm.at[rows], tok.at[s, t], tps.at[0, dp], tpr.at[0, dp], (at(0, dp), t))
    for dp in range(1, q):
        for i, (w, col) in enumerate(((wk, kcol), (wr, rcol))):
            keyp.append(
                push(
                    w.at[:, span(z, LANES)], wts.at[mine, col],
                    kps.at[i * q, dp], kpr.at[i * q, dp], (at(0, dp), t),
                )
            )
    locals_ = [
        local(nrm.at[pl.ds(0, half)], tok.at[s, 0], 0),
        local(nrm.at[pl.ds(half, half)], tok.at[s, 1], 1),
        local(wk.at[:, span(z, LANES)], wts.at[mine, kcol], 2),
        local(wr.at[:, span(z, LANES)], wts.at[mine, rcol], 3),
        local(wv.at[:, mine], wts.at[mine, pl.ds(0, LANES)], 4),
        local(wg.at[:, mine], wts.at[mine, pl.ds(LANES, LANES)], 5),
        local(ws.at[s], wst.at[pl.ds(0, ws.shape[1]), mine], 6),
    ]
    weights = []
    for k in range(1, n):
        j = lax.rem(s + k, n)
        cols = span(j, LANES)
        for i, w in enumerate((wv, wg)):
            weights.append(
                push(w.at[:, cols], wts.at[mine, pl.ds(i * LANES, LANES)], vs.at[k, i], vr.at[k, i], (j, t))
            )
        weights.append(
            push(ws.at[j], wst.at[pl.ds(0, ws.shape[1]), mine], ss.at[k], sr.at[k], (j, t))
        )
    swaps = {}

    def swap(dz, dp):
        src = at(q - dz, q - dp)
        swaps[dz, dp] = push(tok.at[src, t], tok.at[src, t], tss.at[dz, dp], tsr.at[dz, dp], sibling)

    for dz in range(1, q):
        src = at(q - dz, 0)
        first[dz - 1].wait_recv()
        for dp in range(1, q):
            plane[dz, dp] = push(tok.at[src, t], tok.at[src, t], tps.at[dz, dp], tpr.at[dz, dp], (at(0, dp), t))
        swap(dz, 0)
        for copy in keyz[dz - 1]:
            copy.wait_recv()
        got = wts.at[span(src, depth), pl.ds(2 * LANES, 2 * LANES)]
        for dp in range(1, q):
            keyp.append(push(got, got, kps.at[dz, dp], kpr.at[dz, dp], (at(0, dp), t)))
    outs = []
    for dz in range(1, q):
        outs.append(push(wo, wout.at[:, span(z, LANES)], os.at[dz], orr.at[dz], (at(dz, 0), t)))
    locals_.append(local(wo, wout.at[:, span(z, LANES)], 7))

    wst[ws.shape[1] :, :] = jnp.zeros((LANES - ws.shape[1], wst.shape[1]), BF16)
    seq = blocks * BLOCK
    wide = 3 * LANES
    raw[0:8, :] = jnp.zeros((8, wide), F32)
    raw[seq + 8 : seq + 16, :] = jnp.zeros((8, wide), F32)
    for copy in locals_:
        copy.wait()
    for copy in weights + keyp:
        copy.wait_recv()

    def project(plane_index):
        @pl.loop(0, q // 2)
        def _(i):
            chip = plane_index * q + 2 * i
            r0 = pl.multiple_of(chip * BLOCK, 2 * BLOCK)
            at2 = pl.ds(r0, 2 * BLOCK)
            x = tok[pl.ds(chip, 2)].reshape(2 * BLOCK, tok.shape[3])
            got = jnp.dot(x, wts[...], preferred_element_type=F32).astype(BF16)
            for i_, b_ in ((0, 0), (2, 1), (3, 2)):
                raw[pl.ds(r0 + 8, 2 * BLOCK), b_ * LANES : (b_ + 1) * LANES] = got[
                    :, i_ * LANES : (i_ + 1) * LANES
                ].astype(F32)
            gate[at2, :] = got[:, LANES : 2 * LANES]
            u = lax.dot_general(x, wst[...], (((1,), (1,)), ((), ())), preferred_element_type=F32)
            u = u.astype(BF16).astype(F32) + offsets[...]
            pre[at2, :] = jnp.maximum(u, 0.0) + jnp.log1p(jnp.exp(-jnp.abs(u)))

    for dz in range(q):
        for dp in range(1, q):
            plane[dz, dp].wait_recv()
            swap(dz, dp)
        for dp in range(q):
            if (dz, dp) != (0, 0):
                swaps[dz, dp].wait_recv()
        project(lax.rem(z + q - dz, q))

    @pl.loop(0, blocks, unroll=2)
    def _(i):
        r0 = pl.multiple_of(i * BLOCK, BLOCK)
        for b, dst in enumerate((vals, keys, reads)):
            window = raw[pl.ds(r0, BLOCK + 16), b * LANES : (b + 1) * LANES]
            total = jnp.zeros((BLOCK, LANES), F32)
            for k in range(KERNEL):
                lo = 8 - (KERNEL - 1) // 2 + k
                total = total + window[lo : lo + BLOCK] * taps[k : k + 1, b * LANES : (b + 1) * LANES]
            dst[pl.ds(r0, BLOCK), :] = silu(total).astype(BF16)

    ri = lax.broadcasted_iota(jnp.int32, (BLOCK, BLOCK), 0)
    ci = lax.broadcasted_iota(jnp.int32, (BLOCK, BLOCK), 1)
    low = ri >= ci
    diag = ri == ci
    fwd = ci < 2
    left = ci < HEAD_DIM
    lower = jnp.where(low, 1.0, 0.0).astype(F32)
    upper = jnp.where(ri <= ci, 1.0, 0.0).astype(F32)

    @pl.loop(0, blocks, unroll=4)
    def _(i):
        r0 = pl.multiple_of(i * BLOCK, BLOCK)
        here = pl.ds(r0, BLOCK)
        st = pre[here, :]
        ld = -rates[...] * st
        c = jnp.where(
            fwd,
            jnp.dot(lower, ld, precision=FULL_PRECISION, preferred_element_type=F32),
            jnp.dot(upper, ld, precision=FULL_PRECISION, preferred_element_type=F32),
        )
        cums[here, :] = c
        ct = c.T
        stt = st.T
        key, read, val = keys[here, :], reads[here, :], vals[here, :]
        val32 = val.astype(F32)
        score = lax.dot_general(read, key, (((1,), (1,)), ((), ())), preferred_element_type=F32)
        total = jnp.zeros((BLOCK, LANES), F32)
        for h in range(2):
            gap = jnp.where(low, c[:, h : h + 1] - ct[h : h + 1, :], c[:, h + 2 : h + 3] - ct[h + 2 : h + 3, :])
            sb = stt[h + 2 : h + 3, :]
            e = jnp.exp(gap) * jnp.where(low, stt[h : h + 1, :], sb) + jnp.where(diag, sb, 0.0)
            side = left if h == 0 else jnp.logical_not(left)
            own = jnp.where(side, val32, 0.0).astype(BF16)
            total = total + jnp.dot((score * e).astype(BF16), own, preferred_element_type=F32)
        yy[here, :] = total
        c_end = jnp.where(fwd[0:1], c[BLOCK - 1 : BLOCK, :], c[0:1, :])
        weighting = jnp.exp(c_end - c) * st
        key_t = key.astype(F32).T.astype(BF16)
        for d, dst in ((0, injf), (1, injb)):
            w = jnp.where(left, weighting[:, 2 * d : 2 * d + 1], weighting[:, 2 * d + 1 : 2 * d + 2])
            scaled = (val32 * w).astype(BF16)
            dst[i] = jnp.dot(key_t, scaled, preferred_element_type=F32)

    def carry(i, state, d, inj, kept):
        r0 = pl.multiple_of(i * BLOCK, BLOCK)
        here = pl.ds(r0, BLOCK)
        ec = jnp.exp(cums[here, :])
        grown = jnp.where(left, ec[:, 2 * d : 2 * d + 1], ec[:, 2 * d + 1 : 2 * d + 2])
        high = state.astype(BF16)
        rest = (state - high.astype(F32)).astype(BF16)
        read = reads[here, :]
        add = jnp.dot(read, high, preferred_element_type=F32) + jnp.dot(
            read, rest, preferred_element_type=F32
        )
        kept[here, :] = add * grown
        end = grown[BLOCK - 1 : BLOCK, :] if d == 0 else grown[0:1, :]
        return state * end + inj[i]

    def advance(i, states):
        return (
            carry(i, states[0], 0, injf, carf),
            carry(blocks - 1 - i, states[1], 1, injb, carb),
        )

    zero = jnp.zeros((STATE, LANES), F32)
    lax.fori_loop(0, blocks, advance, (zero, zero), unroll=4)

    def finish(i):
        r0 = pl.multiple_of(i * BLOCK, BLOCK)
        here = pl.ds(r0, BLOCK)
        g = (yy[here, :] + carf[here, :] + carb[here, :]) * silu(gate[here, :].astype(F32))
        sq = g * g
        m0 = jnp.sum(jnp.where(left, sq, 0.0), -1, keepdims=True) / HEAD_DIM
        m1 = jnp.sum(jnp.where(left, 0.0, sq), -1, keepdims=True) / HEAD_DIM
        scale = jnp.where(left, lax.rsqrt(m0 + EPSILON), lax.rsqrt(m1 + EPSILON))
        nh[here, :] = (g * scale * gain[...]).astype(BF16)

    away = []
    for dz in range(1, q + 1):
        to = lax.rem(z + dz, q)

        @pl.loop(0, q, unroll=4)
        def _(i):
            finish(to * q + i)

        if dz < q:
            away.append(
                push(nh.at[span(to, q * BLOCK)], full.at[:, mine], as_.at[dz], ar.at[dz], (at(dz, 0), t))
            )
    near = {}
    keep = local(nh.at[span(z, q * BLOCK)], full.at[:, mine], 8)
    for dp in range(1, q):
        near[0, dp] = push(
            nh.at[span(z, q * BLOCK)], full.at[:, mine], bs.at[0, dp], br.at[0, dp], (at(0, dp), t)
        )
    for dz in range(1, q):
        away[dz - 1].wait_recv()
        got = full.at[:, span(at(q - dz, 0), LANES)]
        for dp in range(1, q):
            near[dz, dp] = push(got, got, bs.at[dz, dp], br.at[dz, dp], (at(0, dp), t))
    keep.wait()
    for copy in outs + list(near.values()):
        copy.wait_recv()
    legs = []
    for dp in range(1, q + 1):
        to = lax.rem(p + dp, q)
        part[to] = jnp.dot(full[span(to, BLOCK), :], wout[...], preferred_element_type=F32).astype(BF16)
    for dp in range(1, q):
        to = lax.rem(p + dp, q)
        legs.append(push(part.at[to], both.at[t, p], es.at[dp], er.at[dp], (at(0, dp), t)))
    across = [push(part.at[p], both.at[t, p], fs.at[0], fr.at[0], sibling)]
    keep = local(part.at[p], both.at[t, p], 9)
    for dp in range(1, q):
        legs[dp - 1].wait_recv()
        got = both.at[t, lax.rem(p + q - dp, q)]
        across.append(push(got, got, fs.at[dp], fr.at[dp], sibling))
    keep.wait()
    for copy in across:
        copy.wait()
    for a in range(q):
        for b in range(q):
            here = slice(a * LANES, (a + 1) * LANES)
            total = both[0, b, :, here].astype(F32) + both[1, b, :, here].astype(F32)
            out[:, (a * q + b) * LANES : (a * q + b + 1) * LANES] = total.astype(BF16)
    flat = [copy for pair in keyz for copy in pair]
    for copy in first + flat + list(plane.values()) + keyp + weights + list(swaps.values()):
        copy.wait_send()
    for copy in outs + away + list(near.values()) + legs:
        copy.wait_send()


def whole(n, q, nrm, wv, wg, wk, wr, ws, wo, taps, offsets, rates, gain):
    dma = pltpu.SemaphoreType.DMA
    vm = pltpu.VMEM
    depth = nrm.shape[0]
    width = nrm.shape[1]
    seq = n * depth
    return pl.pallas_call(
        functools.partial(whole_kernel, n, q),
        out_shape=jax.ShapeDtypeStruct((BLOCK, n * LANES), BF16),
        in_specs=[VMEM_SPEC] * 11,
        out_specs=VMEM_SPEC,
        scratch_shapes=[
            vm((n, 2, depth // 2, width), BF16),
            vm((width, 4 * LANES), BF16),
            vm((LANES, width), BF16),
            vm((wo.shape[0], q * LANES), BF16),
            vm((seq + 16, 3 * LANES), F32),
            vm((seq, LANES), BF16),
            vm((seq, LANES), F32),
            vm((seq, LANES), BF16),
            vm((seq, LANES), BF16),
            vm((seq, LANES), BF16),
            vm((seq, LANES), F32),
            vm((seq, LANES), F32),
            vm((seq // BLOCK, STATE, LANES), F32),
            vm((seq // BLOCK, STATE, LANES), F32),
            vm((seq, LANES), F32),
            vm((seq, LANES), F32),
            vm((seq, LANES), BF16),
            vm((q * BLOCK, n * LANES), BF16),
            vm((q, BLOCK, q * LANES), BF16),
            vm((2, q, BLOCK, q * LANES), BF16),
            dma((q,)), dma((q,)), dma((q, q)), dma((q, q)), dma((q, q)), dma((q, q)),
            dma((q, 2)), dma((q, 2)), dma((q + 1, q)), dma((q + 1, q)),
            dma((n, 2)), dma((n, 2)), dma((n,)), dma((n,)), dma((q,)), dma((q,)),
            dma((q,)), dma((q,)), dma((q, q)), dma((q, q)), dma((q,)), dma((q,)),
            dma((q,)), dma((q,)), dma((10,)),
        ],
        compiler_params=pltpu.CompilerParams(
            collective_id=0, has_side_effects=True, vmem_limit_bytes=56 << 20
        ),
        name="whole",
    )(nrm, wv, wg, wk, wr, ws, wo, taps, offsets, rates, gain)


def own_lanes(fwd, bwd, n):
    both = jnp.stack([fwd.reshape(fwd.shape[0], n, -1), bwd.reshape(bwd.shape[0], n, -1)], 2)
    both = both.reshape(fwd.shape[0], n, -1)
    both = jnp.pad(both, ((0, 0), (0, 0), (0, LANES - both.shape[2])))
    return both.transpose(1, 0, 2)


def headwise(
    n,
    q,
    tokens,
    in_gain,
    w_value,
    w_gate,
    w_in_key,
    w_read,
    w_step_fwd,
    w_step_bwd,
    conv_value,
    conv_key,
    conv_read,
    step_bias,
    rate,
    norm_gain,
    w_out,
):
    s = lax.axis_index("sp")
    group = s // q
    nrm = normalize(tokens.astype(F32), in_gain.astype(F32)).astype(BF16)
    steps = own_lanes(w_step_fwd, w_step_bwd, n)[:, :, :16].transpose(0, 2, 1)

    def cut(x, j):
        return lax.dynamic_slice_in_dim(x, j * LANES, LANES, 1)

    taps = jnp.concatenate([cut(conv_value, s), cut(conv_key, group), cut(conv_read, group)], 1)
    small = own_lanes(
        jnp.stack([step_bias[0], rate[0]]), jnp.stack([step_bias[1], rate[1]]), n
    )
    small = lax.dynamic_index_in_dim(small, s, 0, keepdims=False)
    gain = lax.dynamic_slice_in_dim(norm_gain, s * LANES, LANES, 0).astype(F32)[None]
    return whole(
        n, q, nrm, w_value, w_gate, w_in_key, w_read, steps, w_out,
        taps.astype(F32), small[0:1], small[1:2], gain,
    )


def whole_heads(mesh):
    n, q = mesh.shape["sp"], math.isqrt(mesh.shape["sp"])

    def run(*args):
        cols, keys = args[2].shape[1], args[4].shape[1]
        ready = (
            q * q == n
            and mesh.shape["tp"] == 2
            and cols == n * LANES
            and args[14].shape[1] == LANES
            and keys == q * LANES
            and q % 2 == 0
            and args[0].shape[1] == n * LANES
            and args[0].shape[0] == BLOCK
        )
        return headwise(n, q, *args) if ready else body(*args)

    return run


def solution(mesh):
    in_specs = (
        P("sp", None),
        P(),
        P("sp", "tp"),
        P("sp", "tp"),
        P("sp", "tp"),
        P("sp", "tp"),
        P("sp", "tp"),
        P("sp", "tp"),
        P(None, "tp"),
        P(None, "tp"),
        P(None, "tp"),
        P(None, "tp"),
        P(None, "tp"),
        P("tp"),
        P("tp", "sp"),
    )
    out_specs = P("sp", None)
    return jax.shard_map(whole_heads(mesh), mesh=mesh, in_specs=in_specs, out_specs=out_specs, check_vma=False)
```

```python
import functools
import math

import jax
import jax.numpy as jnp
from jax import lax
from jax.experimental import pallas as pl
from jax.experimental.pallas import tpu as pltpu
from jax.sharding import PartitionSpec as P

HEAD_DIM = 64
STATE = 128
KERNEL = 5
BLOCK = 128


EPSILON = 1e-05
FULL_PRECISION = lax.Precision.HIGHEST


def entering_2(x, axis, combine, identity, reverse):
    length, place = (lax.axis_size(axis), lax.axis_index(axis))
    everything = jax.tree.map(lambda part: lax.all_gather(part, axis), x)
    start = jax.tree.map(
        lambda part, zero: jnp.broadcast_to(jnp.asarray(zero, part.dtype), part.shape), x, identity
    )

    def step(k, before):
        at = length - 1 - k if reverse else k
        reached = at > place if reverse else at < place
        new = combine(before, jax.tree.map(lambda part: part[at], everything))
        return jax.tree.map(lambda a, b: jnp.where(reached, a, b), new, before)

    return lax.fori_loop(0, length, step, start)


def with_halo(cells, sides, width):
    for axis, dim in sides:
        count = lax.axis_size(axis)
        ends = count - 1
        head = lax.slice_in_dim(cells, 0, width, axis=dim)
        tail = lax.slice_in_dim(cells, cells.shape[dim] - width, cells.shape[dim], axis=dim)
        cells = jnp.concatenate(
            [
                lax.ppermute(tail, axis, [(i, (i + 1) % count) for i in range(ends)]),
                cells,
                lax.ppermute(head, axis, [((i + 1) % count, i) for i in range(ends)]),
            ],
            axis=dim,
        )
    return cells


def normalize(tensor, gain):
    return tensor * lax.rsqrt(jnp.mean(tensor * tensor, -1, keepdims=True) + EPSILON) * gain


def block_parts(values, step_size, log_decay, in_keys):
    per_group = values.shape[1] // in_keys.shape[1]
    cumulative = jnp.cumsum(log_decay, axis=0)
    log_total = cumulative[-1]
    weighting = jnp.exp(log_total[None, :] - cumulative) * step_size
    key_heads = jnp.repeat(in_keys, per_group, axis=1)
    scaled = (values.astype(jnp.float32) * weighting[:, :, None]).astype(jnp.bfloat16)
    injected = jnp.einsum("jhn,jhp->hpn", key_heads, scaled, preferred_element_type=jnp.float32)
    return (cumulative, jnp.exp(log_total), injected)


def block_step(memory, inputs):
    values, step_size, cumulative, damping, injected, in_keys, read_in = inputs
    per_group = values.shape[1] // in_keys.shape[1]
    scores = jnp.einsum("ign,jgn->ijg", read_in, in_keys, preferred_element_type=jnp.float32)
    scores = jnp.repeat(scores, per_group, axis=2)
    length = values.shape[0]
    below_mask = (jnp.arange(length)[:, None] >= jnp.arange(length)[None, :])[:, :, None]
    gaps = jnp.where(below_mask, cumulative[:, None, :] - cumulative[None, :, :], -jnp.inf)
    weights = (scores * jnp.exp(gaps) * step_size[None, :, :]).astype(jnp.bfloat16)
    within = jnp.einsum("ijh,jhp->ihp", weights, values, preferred_element_type=jnp.float32)
    read_heads = jnp.repeat(read_in.astype(jnp.float32), per_group, axis=1)
    carried = (
        jnp.einsum("ihn,hpn->ihp", read_heads, memory, precision=FULL_PRECISION)
        * jnp.exp(cumulative)[:, :, None]
    )
    memory = damping[:, None, None] * memory + injected
    return (memory, within + carried)


def blocked(tensor):
    blocks = tensor.shape[0] // BLOCK
    return tensor.reshape((blocks, BLOCK) + tensor.shape[1:])


def sweep(block_inputs, memory):
    memory, swept = lax.scan(block_step, memory, block_inputs)
    return (swept.reshape((swept.shape[0] * swept.shape[1],) + swept.shape[2:]), memory)


def settle(damping_blocks, injected_blocks, memory):

    def advance(memory, inputs):
        return (inputs[0][:, None, None] * memory + inputs[1], None)

    memory, unused = lax.scan(advance, memory, (damping_blocks, injected_blocks))
    return memory


def chain(before_pair, after_pair):
    return (
        before_pair[0] * after_pair[0],
        after_pair[0][:, None, None] * before_pair[1] + after_pair[1],
    )


def entering(damping, final_state, backward):
    identity_pair = (jnp.ones_like(damping), jnp.zeros_like(final_state))
    if backward:
        arrived = entering_2((damping, final_state), "sp", chain, identity_pair, True)
    else:
        arrived = entering_2((damping, final_state), "sp", chain, identity_pair, False)
    return arrived[1]


def body(
    tokens,
    in_gain,
    w_value,
    w_gate,
    w_in_key,
    w_read,
    w_step_fwd,
    w_step_bwd,
    conv_value,
    conv_key,
    conv_read,
    step_bias,
    rate,
    norm_gain,
    w_out,
):
    normed = normalize(tokens.astype(jnp.float32), in_gain.astype(jnp.float32)).astype(jnp.bfloat16)
    weights = (
        lax.all_gather(w_value, "sp", axis=0, tiled=True),
        lax.all_gather(w_gate, "sp", axis=0, tiled=True),
        lax.all_gather(w_in_key, "sp", axis=0, tiled=True),
        lax.all_gather(w_read, "sp", axis=0, tiled=True),
        lax.all_gather(w_step_fwd, "sp", axis=0, tiled=True),
        lax.all_gather(w_step_bwd, "sp", axis=0, tiled=True),
    )
    projected = [
        jnp.dot(normed, weight, preferred_element_type=jnp.float32).astype(jnp.bfloat16)
        for weight in weights
    ]
    value_raw, gate_raw, key_raw, read_raw, pre_fwd, pre_bwd = projected
    value_cols = value_raw.shape[1]
    key_cols = key_raw.shape[1]
    joined = jnp.concatenate([value_raw, key_raw, read_raw], axis=1)
    padded = with_halo(joined, (("sp", 0),), (KERNEL - 1) // 2)
    kernel_taps = jnp.concatenate([conv_value, conv_key, conv_read], axis=1).astype(jnp.float32)
    length = joined.shape[0]
    summed = jnp.zeros(joined.shape, jnp.float32)
    for offset in range(KERNEL):
        summed = summed + padded[offset : offset + length].astype(jnp.float32) * kernel_taps[offset]
    mixed_in = jax.nn.silu(summed).astype(jnp.bfloat16)
    head_count = value_cols // HEAD_DIM
    group_count = key_cols // STATE
    values = mixed_in[:, :value_cols].reshape(length, head_count, HEAD_DIM)
    in_keys = mixed_in[:, value_cols : value_cols + key_cols].reshape(length, group_count, STATE)
    read_in = mixed_in[:, value_cols + key_cols :].reshape(length, group_count, STATE)
    blank = jnp.zeros((head_count, HEAD_DIM, STATE), jnp.float32)
    summed_heads = jnp.zeros(values.shape, jnp.float32)
    for direction, step_pre in ((0, pre_fwd), (1, pre_bwd)):
        step_size = jax.nn.softplus(step_pre.astype(jnp.float32) + step_bias[direction])
        log_decay = -rate[direction] * step_size
        ordered = (values, step_size, log_decay, in_keys, read_in)
        if direction == 1:
            ordered = tuple((tensor[::-1] for tensor in ordered))
        value_blocks, step_blocks, decay_blocks, key_blocks, read_blocks = [
            blocked(tensor) for tensor in ordered
        ]
        cumulative_blocks, damping_blocks, injected_blocks = jax.vmap(block_parts)(
            value_blocks, step_blocks, decay_blocks, key_blocks
        )
        block_inputs = (
            value_blocks,
            step_blocks,
            cumulative_blocks,
            damping_blocks,
            injected_blocks,
            key_blocks,
            read_blocks,
        )
        damping = jnp.exp(jnp.sum(ordered[2], axis=0))
        final_state = settle(damping_blocks, injected_blocks, blank)
        arriving = entering(damping, final_state, direction == 1)
        swept, final_state = sweep(block_inputs, arriving)
        if direction == 1:
            swept = swept[::-1]
        summed_heads = summed_heads + swept
    gated_out = summed_heads * jax.nn.silu(gate_raw.astype(jnp.float32)).reshape(values.shape)
    head_gain = norm_gain.astype(jnp.float32).reshape(head_count, HEAD_DIM)
    normed_heads = normalize(gated_out, head_gain).astype(jnp.bfloat16).reshape(length, value_cols)
    out_whole = lax.all_gather(w_out, "sp", axis=1, tiled=True)
    own_rows = lax.psum_scatter(
        jnp.dot(normed_heads, out_whole, preferred_element_type=jnp.float32).astype(jnp.bfloat16),
        "tp",
        scatter_dimension=0,
        tiled=True,
    )
    return lax.all_gather(own_rows, "tp", axis=0, tiled=True)


F32 = jnp.float32
BF16 = jnp.bfloat16
LANES = 128
VMEM_SPEC = pl.BlockSpec(memory_space=pltpu.VMEM)


def greet(peers):
    barrier = pltpu.get_barrier_semaphore()
    for peer in peers:
        pl.semaphore_signal(
            barrier, inc=1, device_id=peer, device_id_type=pl.DeviceIdType.MESH
        )
    pl.semaphore_wait(barrier, len(peers))


def push(src, dst, send, recv, peer):
    copy = pltpu.make_async_remote_copy(
        src_ref=src,
        dst_ref=dst,
        send_sem=send,
        recv_sem=recv,
        device_id=peer,
        device_id_type=pl.DeviceIdType.MESH,
    )
    copy.start()
    return copy


def silu(x):
    return x * jax.nn.sigmoid(x)


def whole_kernel(
    n, q, nrm, wv, wg, wk, wr, ws, wo, taps, offsets, rates, gain, out,
    tok, wts, wst, wout, raw, gate, pre, vals, keys, reads, cums, yy, injf, injb, carf, carb, nh, full, part, both,
    tzs, tzr, tps, tpr, tss, tsr, kzs, kzr, kps, kpr, vs, vr, ss, sr, os, orr,
    as_, ar, bs, br, es, er, fs, fr, ls,
):
    s, t = lax.axis_index("sp"), lax.axis_index("tp")
    z, p = s // q, s % q
    sibling = (s, 1 - t)
    half = tok.shape[2]
    depth = wv.shape[0]
    blocks = tok.shape[0] * 2 * half // BLOCK

    def at(dz, dp):
        return lax.rem(z + dz, q) * q + lax.rem(p + dp, q)

    def span(i, size):
        return pl.ds(pl.multiple_of(i * size, size), size)

    px = p + 1 - 2 * lax.rem(p, 2)
    py = lax.rem(p + 2, q)
    pd = lax.rem(px + 2, q)
    side = {"x": (z * q + px, t), "y": (z * q + py, t)}

    def chip(dz, where):
        return lax.rem(z + q - dz, q) * q + where

    greet([(lax.rem(s + k, n), t) for k in range(1, n)] + [sibling])

    def local(src, dst, i):
        copy = pltpu.make_async_copy(src, dst, ls.at[i])
        copy.start()
        return copy

    mine = span(s, depth)
    rows = span(t, half)
    kcol, rcol = pl.ds(2 * LANES, LANES), pl.ds(3 * LANES, LANES)
    first, keyz = [], []
    for dz in range(1, q):
        first.append(push(nrm.at[rows], tok.at[s, t], tzs.at[dz], tzr.at[dz], (at(dz, 0), t)))
    for dz in range(1, q):
        grp = span(lax.rem(z + dz, q), LANES)
        keyz.append(
            [
                push(w.at[:, grp], wts.at[mine, col], kzs.at[dz, i], kzr.at[dz, i], (at(dz, 0), t))
                for i, (w, col) in enumerate(((wk, kcol), (wr, rcol)))
            ]
        )
    plane, keyp = {}, []
    for i, to in enumerate("xy"):
        plane[0, to] = push(nrm.at[rows], tok.at[s, t], tps.at[0, i], tpr.at[0, i], side[to])
    for dp in range(1, q):
        for i, (w, col) in enumerate(((wk, kcol), (wr, rcol))):
            keyp.append(
                push(
                    w.at[:, span(z, LANES)], wts.at[mine, col],
                    kps.at[i * q, dp], kpr.at[i * q, dp], (at(0, dp), t),
                )
            )
    locals_ = [
        local(nrm.at[pl.ds(0, half)], tok.at[s, 0], 0),
        local(nrm.at[pl.ds(half, half)], tok.at[s, 1], 1),
        local(wk.at[:, span(z, LANES)], wts.at[mine, kcol], 2),
        local(wr.at[:, span(z, LANES)], wts.at[mine, rcol], 3),
        local(wv.at[:, mine], wts.at[mine, pl.ds(0, LANES)], 4),
        local(wg.at[:, mine], wts.at[mine, pl.ds(LANES, LANES)], 5),
        local(ws.at[s], wst.at[pl.ds(0, ws.shape[1]), mine], 6),
    ]
    weights = []
    for k in range(1, n):
        j = lax.rem(s + k, n)
        cols = span(j, LANES)
        for i, w in enumerate((wv, wg)):
            weights.append(
                push(w.at[:, cols], wts.at[mine, pl.ds(i * LANES, LANES)], vs.at[k, i], vr.at[k, i], (j, t))
            )
        weights.append(
            push(ws.at[j], wst.at[pl.ds(0, ws.shape[1]), mine], ss.at[k], sr.at[k], (j, t))
        )
    swaps = {}

    def swap(dz, i):
        src = chip(dz, (p, px, py, pd)[i])
        swaps[dz, i] = push(tok.at[src, t], tok.at[src, t], tss.at[dz, i], tsr.at[dz, i], sibling)

    for dz in range(1, q):
        src = at(q - dz, 0)
        first[dz - 1].wait_recv()
        for i, to in enumerate("xy"):
            plane[dz, to] = push(tok.at[src, t], tok.at[src, t], tps.at[dz, i], tpr.at[dz, i], side[to])
        swap(dz, 0)
        for copy in keyz[dz - 1]:
            copy.wait_recv()
        got = wts.at[span(src, depth), pl.ds(2 * LANES, 2 * LANES)]
        for dp in range(1, q):
            keyp.append(push(got, got, kps.at[dz, dp], kpr.at[dz, dp], (at(0, dp), t)))
    outs = []
    for dz in range(1, q):
        outs.append(push(wo, wout.at[:, span(z, LANES)], os.at[dz], orr.at[dz], (at(dz, 0), t)))
    locals_.append(local(wo, wout.at[:, span(z, LANES)], 7))

    wst[ws.shape[1] :, :] = jnp.zeros((LANES - ws.shape[1], wst.shape[1]), BF16)
    seq = blocks * BLOCK
    wide = 3 * LANES
    raw[0:8, :] = jnp.zeros((8, wide), F32)
    raw[seq + 8 : seq + 16, :] = jnp.zeros((8, wide), F32)
    for copy in locals_:
        copy.wait()

    def project(plane_index):
        @pl.loop(0, q // 2)
        def _(i):
            pair = plane_index * q + 2 * i
            r0 = pl.multiple_of(pair * BLOCK, 2 * BLOCK)
            at2 = pl.ds(r0, 2 * BLOCK)
            x = tok[pl.ds(pair, 2)].reshape(2 * BLOCK, tok.shape[3])
            got = jnp.dot(x, wts[...], preferred_element_type=F32).astype(BF16)
            for i_, b_ in ((0, 0), (2, 1), (3, 2)):
                raw[pl.ds(r0 + 8, 2 * BLOCK), b_ * LANES : (b_ + 1) * LANES] = got[
                    :, i_ * LANES : (i_ + 1) * LANES
                ].astype(F32)
            gate[at2, :] = got[:, LANES : 2 * LANES]
            u = lax.dot_general(x, wst[...], (((1,), (1,)), ((), ())), preferred_element_type=F32)
            u = u.astype(BF16).astype(F32) + offsets[...]
            pre[at2, :] = jnp.maximum(u, 0.0) + jnp.log1p(jnp.exp(-jnp.abs(u)))

    quarter = half // 2

    def relay(dz):
        for i, (near_by, other) in enumerate((("x", "y"), ("y", "x"))):
            plane[dz, near_by].wait_recv()
            got = tok.at[chip(dz, (px, py)[i]), t, pl.ds(i * quarter, quarter)]
            plane[dz, other + "d"] = push(got, got, tps.at[dz, 2 + i], tpr.at[dz, 2 + i], side[other])
            swap(dz, 1 + i)

    def use(dz):
        plane[dz, "yd"].wait_recv()
        plane[dz, "xd"].wait_recv()
        swap(dz, 3)
        for i in range(q):
            if (dz, i) != (0, 0):
                swaps[dz, i].wait_recv()
        project(lax.rem(z + q - dz, q))

    for dz in range(q):
        relay(dz)
        if dz == 1:
            for copy in weights + keyp:
                copy.wait_recv()
        if dz >= 1:
            use(dz - 1)
    use(q - 1)

    @pl.loop(0, blocks, unroll=2)
    def _(i):
        r0 = pl.multiple_of(i * BLOCK, BLOCK)
        for b, dst in enumerate((vals, keys, reads)):
            window = raw[pl.ds(r0, BLOCK + 16), b * LANES : (b + 1) * LANES]
            total = jnp.zeros((BLOCK, LANES), F32)
            for k in range(KERNEL):
                lo = 8 - (KERNEL - 1) // 2 + k
                total = total + window[lo : lo + BLOCK] * taps[k : k + 1, b * LANES : (b + 1) * LANES]
            dst[pl.ds(r0, BLOCK), :] = silu(total).astype(BF16)

    ri = lax.broadcasted_iota(jnp.int32, (BLOCK, BLOCK), 0)
    ci = lax.broadcasted_iota(jnp.int32, (BLOCK, BLOCK), 1)
    low = ri >= ci
    diag = ri == ci
    fwd = ci < 2
    left = ci < HEAD_DIM
    lower = jnp.where(low, 1.0, 0.0).astype(F32)
    upper = jnp.where(ri <= ci, 1.0, 0.0).astype(F32)

    @pl.loop(0, blocks, unroll=4)
    def _(i):
        r0 = pl.multiple_of(i * BLOCK, BLOCK)
        here = pl.ds(r0, BLOCK)
        st = pre[here, :]
        ld = -rates[...] * st
        c = jnp.where(
            fwd,
            jnp.dot(lower, ld, precision=FULL_PRECISION, preferred_element_type=F32),
            jnp.dot(upper, ld, precision=FULL_PRECISION, preferred_element_type=F32),
        )
        cums[here, :] = c
        ct = c.T
        stt = st.T
        key, read, val = keys[here, :], reads[here, :], vals[here, :]
        val32 = val.astype(F32)
        score = lax.dot_general(read, key, (((1,), (1,)), ((), ())), preferred_element_type=F32)
        total = jnp.zeros((BLOCK, LANES), F32)
        for h in range(2):
            gap = jnp.where(low, c[:, h : h + 1] - ct[h : h + 1, :], c[:, h + 2 : h + 3] - ct[h + 2 : h + 3, :])
            sb = stt[h + 2 : h + 3, :]
            e = jnp.exp(gap) * jnp.where(low, stt[h : h + 1, :], sb) + jnp.where(diag, sb, 0.0)
            mask = left if h == 0 else jnp.logical_not(left)
            own = jnp.where(mask, val32, 0.0).astype(BF16)
            total = total + jnp.dot((score * e).astype(BF16), own, preferred_element_type=F32)
        yy[here, :] = total
        c_end = jnp.where(fwd[0:1], c[BLOCK - 1 : BLOCK, :], c[0:1, :])
        weighting = jnp.exp(c_end - c) * st
        key_t = key.astype(F32).T.astype(BF16)
        for d, dst in ((0, injf), (1, injb)):
            w = jnp.where(left, weighting[:, 2 * d : 2 * d + 1], weighting[:, 2 * d + 1 : 2 * d + 2])
            scaled = (val32 * w).astype(BF16)
            dst[i] = jnp.dot(key_t, scaled, preferred_element_type=F32)

    def carry(i, state, d, inj, kept):
        r0 = pl.multiple_of(i * BLOCK, BLOCK)
        here = pl.ds(r0, BLOCK)
        ec = jnp.exp(cums[here, :])
        grown = jnp.where(left, ec[:, 2 * d : 2 * d + 1], ec[:, 2 * d + 1 : 2 * d + 2])
        high = state.astype(BF16)
        rest = (state - high.astype(F32)).astype(BF16)
        read = reads[here, :]
        add = jnp.dot(read, high, preferred_element_type=F32) + jnp.dot(
            read, rest, preferred_element_type=F32
        )
        kept[here, :] = add * grown
        end = grown[BLOCK - 1 : BLOCK, :] if d == 0 else grown[0:1, :]
        return state * end + inj[i]

    def advance(i, states):
        return (
            carry(i, states[0], 0, injf, carf),
            carry(blocks - 1 - i, states[1], 1, injb, carb),
        )

    zero = jnp.zeros((STATE, LANES), F32)
    lax.fori_loop(0, blocks, advance, (zero, zero), unroll=4)

    def finish(i):
        r0 = pl.multiple_of(i * BLOCK, BLOCK)
        here = pl.ds(r0, BLOCK)
        g = (yy[here, :] + carf[here, :] + carb[here, :]) * silu(gate[here, :].astype(F32))
        sq = g * g
        m0 = jnp.sum(jnp.where(left, sq, 0.0), -1, keepdims=True) / HEAD_DIM
        m1 = jnp.sum(jnp.where(left, 0.0, sq), -1, keepdims=True) / HEAD_DIM
        scale = jnp.where(left, lax.rsqrt(m0 + EPSILON), lax.rsqrt(m1 + EPSILON))
        nh[here, :] = (g * scale * gain[...]).astype(BF16)

    away = []
    for dz in range(1, q + 1):
        to = lax.rem(z + dz, q)

        @pl.loop(0, q, unroll=4)
        def _(i):
            finish(to * q + i)

        if dz < q:
            away.append(
                push(nh.at[span(to, q * BLOCK)], full.at[:, mine], as_.at[dz], ar.at[dz], (at(dz, 0), t))
            )
    near = {}
    keep = local(nh.at[span(z, q * BLOCK)], full.at[:, mine], 8)
    for i, to in enumerate("xy"):
        near[0, to] = push(
            nh.at[span(z, q * BLOCK)], full.at[:, mine], bs.at[0, i], br.at[0, i], side[to]
        )
    for dz in range(1, q):
        away[dz - 1].wait_recv()
        got = full.at[:, span(at(q - dz, 0), LANES)]
        for i, to in enumerate("xy"):
            near[dz, to] = push(got, got, bs.at[dz, i], br.at[dz, i], side[to])
    rest_rows = q * BLOCK // 2
    for dz in range(q):
        for i, (near_by, other) in enumerate((("x", "y"), ("y", "x"))):
            near[dz, near_by].wait_recv()
            got = full.at[pl.ds(i * rest_rows, rest_rows), span(chip(dz, (px, py)[i]), LANES)]
            near[dz, other + "d"] = push(got, got, bs.at[dz, 2 + i], br.at[dz, 2 + i], side[other])
    keep.wait()
    for copy in outs + [near[dz, to] for dz in range(q) for to in ("xd", "yd")]:
        copy.wait_recv()
    legs = []
    for dp in range(1, q + 1):
        to = lax.rem(p + dp, q)
        part[to] = jnp.dot(full[span(to, BLOCK), :], wout[...], preferred_element_type=F32).astype(BF16)
    for dp in range(1, q):
        to = lax.rem(p + dp, q)
        legs.append(push(part.at[to], both.at[t, p], es.at[dp], er.at[dp], (at(0, dp), t)))
    across = [push(part.at[p], both.at[t, p], fs.at[0], fr.at[0], sibling)]
    keep = local(part.at[p], both.at[t, p], 9)
    for dp in range(1, q):
        legs[dp - 1].wait_recv()
        got = both.at[t, lax.rem(p + q - dp, q)]
        across.append(push(got, got, fs.at[dp], fr.at[dp], sibling))
    keep.wait()
    for copy in across:
        copy.wait()
    for a in range(q):
        for b in range(q):
            here = slice(a * LANES, (a + 1) * LANES)
            total = both[0, b, :, here].astype(F32) + both[1, b, :, here].astype(F32)
            out[:, (a * q + b) * LANES : (a * q + b + 1) * LANES] = total.astype(BF16)
    flat = [copy for pair in keyz for copy in pair]
    for copy in first + flat + list(plane.values()) + keyp + weights + list(swaps.values()):
        copy.wait_send()
    for copy in outs + away + list(near.values()) + legs:
        copy.wait_send()


def whole(n, q, nrm, wv, wg, wk, wr, ws, wo, taps, offsets, rates, gain):
    dma = pltpu.SemaphoreType.DMA
    vm = pltpu.VMEM
    depth = nrm.shape[0]
    width = nrm.shape[1]
    seq = n * depth
    return pl.pallas_call(
        functools.partial(whole_kernel, n, q),
        out_shape=jax.ShapeDtypeStruct((BLOCK, n * LANES), BF16),
        in_specs=[VMEM_SPEC] * 11,
        out_specs=VMEM_SPEC,
        scratch_shapes=[
            vm((n, 2, depth // 2, width), BF16),
            vm((width, 4 * LANES), BF16),
            vm((LANES, width), BF16),
            vm((wo.shape[0], q * LANES), BF16),
            vm((seq + 16, 3 * LANES), F32),
            vm((seq, LANES), BF16),
            vm((seq, LANES), F32),
            vm((seq, LANES), BF16),
            vm((seq, LANES), BF16),
            vm((seq, LANES), BF16),
            vm((seq, LANES), F32),
            vm((seq, LANES), F32),
            vm((seq // BLOCK, STATE, LANES), F32),
            vm((seq // BLOCK, STATE, LANES), F32),
            vm((seq, LANES), F32),
            vm((seq, LANES), F32),
            vm((seq, LANES), BF16),
            vm((q * BLOCK, n * LANES), BF16),
            vm((q, BLOCK, q * LANES), BF16),
            vm((2, q, BLOCK, q * LANES), BF16),
            dma((q,)), dma((q,)), dma((q, q)), dma((q, q)), dma((q, q)), dma((q, q)),
            dma((q, 2)), dma((q, 2)), dma((q + 1, q)), dma((q + 1, q)),
            dma((n, 2)), dma((n, 2)), dma((n,)), dma((n,)), dma((q,)), dma((q,)),
            dma((q,)), dma((q,)), dma((q, q)), dma((q, q)), dma((q,)), dma((q,)),
            dma((q,)), dma((q,)), dma((10,)),
        ],
        compiler_params=pltpu.CompilerParams(
            collective_id=0, has_side_effects=True, vmem_limit_bytes=56 << 20
        ),
        name="whole",
    )(nrm, wv, wg, wk, wr, ws, wo, taps, offsets, rates, gain)


def own_lanes(fwd, bwd, n):
    both = jnp.stack([fwd.reshape(fwd.shape[0], n, -1), bwd.reshape(bwd.shape[0], n, -1)], 2)
    both = both.reshape(fwd.shape[0], n, -1)
    both = jnp.pad(both, ((0, 0), (0, 0), (0, LANES - both.shape[2])))
    return both.transpose(1, 0, 2)


def headwise(
    n,
    q,
    tokens,
    in_gain,
    w_value,
    w_gate,
    w_in_key,
    w_read,
    w_step_fwd,
    w_step_bwd,
    conv_value,
    conv_key,
    conv_read,
    step_bias,
    rate,
    norm_gain,
    w_out,
):
    s = lax.axis_index("sp")
    group = s // q
    nrm = normalize(tokens.astype(F32), in_gain.astype(F32)).astype(BF16)
    steps = own_lanes(w_step_fwd, w_step_bwd, n)[:, :, :16].transpose(0, 2, 1)

    def cut(x, j):
        return lax.dynamic_slice_in_dim(x, j * LANES, LANES, 1)

    taps = jnp.concatenate([cut(conv_value, s), cut(conv_key, group), cut(conv_read, group)], 1)
    small = own_lanes(
        jnp.stack([step_bias[0], rate[0]]), jnp.stack([step_bias[1], rate[1]]), n
    )
    small = lax.dynamic_index_in_dim(small, s, 0, keepdims=False)
    gain = lax.dynamic_slice_in_dim(norm_gain, s * LANES, LANES, 0).astype(F32)[None]
    return whole(
        n, q, nrm, w_value, w_gate, w_in_key, w_read, steps, w_out,
        taps.astype(F32), small[0:1], small[1:2], gain,
    )


def whole_heads(mesh):
    n, q = mesh.shape["sp"], math.isqrt(mesh.shape["sp"])

    def run(*args):
        cols, keys = args[2].shape[1], args[4].shape[1]
        ready = (
            q * q == n
            and mesh.shape["tp"] == 2
            and cols == n * LANES
            and args[14].shape[1] == LANES
            and keys == q * LANES
            and q == 4
            and args[0].shape[1] == n * LANES
            and args[0].shape[0] == BLOCK
        )
        return headwise(n, q, *args) if ready else body(*args)

    return run


def solution(mesh):
    in_specs = (
        P("sp", None),
        P(),
        P("sp", "tp"),
        P("sp", "tp"),
        P("sp", "tp"),
        P("sp", "tp"),
        P("sp", "tp"),
        P("sp", "tp"),
        P(None, "tp"),
        P(None, "tp"),
        P(None, "tp"),
        P(None, "tp"),
        P(None, "tp"),
        P("tp"),
        P("tp", "sp"),
    )
    out_specs = P("sp", None)
    return jax.shard_map(whole_heads(mesh), mesh=mesh, in_specs=in_specs, out_specs=out_specs, check_vma=False)
```
